512 devices in a mesh: sp: 16 (over z), fs: 4 (over y), tp: 8 (over x, core).
Axes of the slice: x: 4, y: 4, z: 16, core: 2. Of those that a mesh axis runs over, the one named last changes fastest.
Arguments:
- tokens: bfloat16 [4, 8192, 2048], P('fs', ('sp', 'tp')), may hold values from -6 to 6
- input_gain: float32 [2048], replicated, may hold values from 0.1 to 1.9
- query_weight: bfloat16 [2048, 768], P(None, 'tp'), may hold values from -0.125 to 0.125
- latent_down: bfloat16 [2048, 256], replicated, may hold values from -0.125 to 0.125
- rotary_down: bfloat16 [2048, 32], replicated, may hold values from -0.125 to 0.125
- pool_down: bfloat16 [2048, 1024], P(None, 'tp'), may hold values from -0.125 to 0.125
- key_up: bfloat16 [256, 512], replicated, may hold values from -0.375 to 0.375
- value_up: bfloat16 [256, 1024], replicated, may hold values from -1.125 to 1.125, as said below
- query_gain: float32 [96], replicated, may hold values from 0.1 to 1.9
- key_gain: float32 [96], replicated, may hold values from 0.1 to 1.9
- pool_weight: bfloat16 [16, 64, 64], replicated, may hold values from -2.25 to 2.25, as said below
- pool_scale: float32 [1024], P('tp'), may hold values from 0.1 to 1.9
- attention_gain: float32 [1024], P('tp'), may hold values from 0.1 to 1.9
- pool_gain: float32 [1024], P('tp'), may hold values from 0.1 to 1.9
- attention_out: bfloat16 [1024, 2048], P('tp'), may hold values from -0.125 to 0.125
- pool_out: bfloat16 [1024, 2048], P('tp'), may hold values from -0.125 to 0.125
Outputs:
- mixed: bfloat16 [4, 8192, 2048], P('fs', ('sp', 'tp'))
The draws below stay inside these ranges and needn't reach their ends.
Inputs may be any that keep to these rules, and one draw needn't show every extreme that they name: `value_up`: entries of order 256 ** -0.5 or larger. `pool_weight`: entries of order 64 ** -0.5 or larger.
All inputs are finite; a program needn't handle non-finite values.
Results may differ from the reference program's by a relative error of at most 0.015.
Values may be sent and summed in bfloat16 or wider, within the bound.
No kernel may reach another device: no remote copies, remote signals or barrier semaphores. Data moves between devices by JAX's collectives and lax.ppermute only.
A program may use at most 64 MiB of HBM per device.

```python
import math
import jax
import jax.numpy as jnp
from jax import lax

D = 2048
HEADS = 8
NOPE_DIM = 64
ROPE_DIM = 32
VALUE_DIM = 128
KV_LATENT = 256
GROUPS = 16
GROUP_DIM = 64
QK_DIM = 96
POOL_WIDTH = 1024
SEQS = 4
LENGTH = 8192
HEAD_BLOCKS = 8


def draw_value_up(key, part):
    columns = jnp.arange(HEADS * VALUE_DIM, dtype=jnp.int32) // VALUE_DIM
    level = columns.astype(jnp.float32) / (HEADS - 1)
    base = jnp.clip(jax.random.normal(key, (KV_LATENT, HEADS * VALUE_DIM), jnp.float32), -6.0, 6.0)
    factor = 3.0 ** level
    return (base * factor[None, :] * KV_LATENT ** (-0.5)).astype(jnp.bfloat16)


def draw_pool_weight(key, part):
    level = jnp.arange(GROUPS, dtype=jnp.int32).astype(jnp.float32) / (GROUPS - 1)
    base = jnp.clip(jax.random.normal(key, (GROUPS, GROUP_DIM, GROUP_DIM), jnp.float32), -6.0, 6.0)
    factor = 3.0 ** level
    return (base * factor[:, None, None] * GROUP_DIM ** (-0.5)).astype(jnp.bfloat16)


def steps_of(stream_key, shape, split, least, high):
    def one(position, blocks):
        draws = jax.random.uniform(jax.random.fold_in(jax.random.fold_in(stream_key, 6), position), (blocks,), jnp.float32, least / len(split), high / len(split))
        return jnp.repeat(jnp.exp(draws), shape[position] // blocks).reshape((-1,) + (1,) * (len(shape) - position - 1))

    factor_of = one(*split[0])
    for cut in split[1:]:
        factor_of = factor_of * one(*cut)
    return factor_of


def centred(key, extent, deviation, bound, pieces=(), kind=jnp.bfloat16):
    entries = deviation * jax.random.normal(key, extent, jnp.float32)
    if pieces:
        entries = entries * steps_of(key, extent, pieces, -0.22, 0.18)
    return jnp.clip(entries, -bound, bound).astype(kind)


def setup_inputs(seed: int = 0) -> dict:
    streams_of = jax.random.split(jax.random.key(seed), 17)
    tokens = centred(streams_of[0], (SEQS, LENGTH, D), 1.0, 6.0, ((0, 4), (1, 128)))
    input_gain = jnp.clip(1.0 + 0.18 * jax.random.normal(streams_of[1], (D,), jnp.float32), 0.1, 1.9)
    query_weight = centred(streams_of[2], (D, HEADS * QK_DIM), D ** -0.5, 0.125, ((1, 8),))
    latent_down = centred(streams_of[3], (D, KV_LATENT), D ** -0.5, 0.125)
    rotary_down = centred(streams_of[4], (D, ROPE_DIM), D ** -0.5, 0.125)
    pool_down = centred(streams_of[5], (D, POOL_WIDTH), D ** -0.5, 0.125, ((1, 8),))
    key_up = centred(streams_of[6], (KV_LATENT, HEADS * NOPE_DIM), KV_LATENT ** -0.5, 0.375)
    value_up = draw_value_up(jax.random.fold_in(streams_of[16], 71), 0)
    query_gain = jnp.clip(1.0 + 0.18 * jax.random.normal(streams_of[8], (QK_DIM,), jnp.float32), 0.1, 1.9)
    key_gain = jnp.clip(1.0 + 0.18 * jax.random.normal(streams_of[9], (QK_DIM,), jnp.float32), 0.1, 1.9)
    pool_weight = draw_pool_weight(jax.random.fold_in(streams_of[16], 71), 0)
    pool_scale = jnp.clip(1.0 + 0.18 * jax.random.normal(streams_of[11], (POOL_WIDTH,), jnp.float32), 0.1, 1.9)
    attention_gain = jnp.clip(1.0 + 0.18 * jax.random.normal(streams_of[12], (HEADS * VALUE_DIM,), jnp.float32), 0.1, 1.9)
    pool_gain = jnp.clip(1.0 + 0.18 * jax.random.normal(streams_of[13], (POOL_WIDTH,), jnp.float32), 0.1, 1.9)
    attention_out = centred(streams_of[14], (HEADS * VALUE_DIM, D), (HEADS * VALUE_DIM + POOL_WIDTH) ** -0.5, 0.125, ((0, 8),))
    pool_out = centred(streams_of[15], (POOL_WIDTH, D), (HEADS * VALUE_DIM + POOL_WIDTH) ** -0.5, 0.125, ((0, 8),))
    return {"tokens": tokens, "input_gain": input_gain, "query_weight": query_weight, "latent_down": latent_down, "rotary_down": rotary_down, "pool_down": pool_down, "key_up": key_up, "value_up": value_up, "query_gain": query_gain, "key_gain": key_gain, "pool_weight": pool_weight, "pool_scale": pool_scale, "attention_gain": attention_gain, "pool_gain": pool_gain, "attention_out": attention_out, "pool_out": pool_out}


EPS = 1e-06
THETA = 10000.0
rim_rows = 16

def rms_scale(values):
    return lax.rsqrt(lax.optimization_barrier(jnp.mean(values * values, axis=-1, keepdims=True)) + EPS)

def rotate(values, positions):
    half = values.shape[-1] // 2
    inv_freq = 1.0 / THETA ** (jnp.arange(half, dtype=jnp.float32) / half)
    angle = positions[:, None, None] * inv_freq
    cosine = jnp.cos(angle)
    sine = jnp.sin(angle)
    first = values[..., :half]
    second = values[..., half:]
    return jnp.concatenate([first * cosine - second * sine, second * cosine + first * sine], axis=-1)

def head_vectors(raw, gain, positions):
    normal = raw * rms_scale(raw) * gain
    turned = rotate(normal[..., NOPE_DIM:], positions)
    return jnp.concatenate([normal[..., :NOPE_DIM], turned], axis=-1).astype(jnp.bfloat16)

def expand_keys(latent_rows, first, key_up, value_up, key_gain):
    count = latent_rows.shape[0]
    heads = key_up.shape[1] // NOPE_DIM
    latent = latent_rows[:, :KV_LATENT].astype(jnp.float32)
    latent_normed = (latent * rms_scale(latent)).astype(jnp.bfloat16)
    plain = jnp.dot(latent_normed, key_up, preferred_element_type=jnp.float32).reshape(count, heads, NOPE_DIM)
    values = jnp.dot(latent_normed, value_up, preferred_element_type=jnp.float32).astype(jnp.bfloat16)
    shared = latent_rows[:, KV_LATENT:].astype(jnp.float32)
    shared = jnp.broadcast_to(shared[:, None, :], (count, heads, ROPE_DIM))
    positions = (first + jnp.arange(count, dtype=jnp.int32)).astype(jnp.float32)
    keys = head_vectors(jnp.concatenate([plain, shared], axis=-1), key_gain, positions)
    return (keys, values.reshape(count, heads, VALUE_DIM))

def pool_mix(pool_input, before, group_ids, positions):
    count = pool_input.shape[0]
    groups = group_ids.shape[0]
    current = pool_input.astype(jnp.float32).reshape(count, groups, GROUP_DIM)
    extended = jnp.concatenate([before, pool_input], axis=0).astype(jnp.float32)
    extended = extended.reshape(count + rim_rows, groups, GROUP_DIM)
    window = jnp.left_shift(2, group_ids % 4).astype(jnp.float32)
    total = current
    for back in range(1, rim_rows):
        taken = (window > back).astype(jnp.float32)
        total = total + extended[rim_rows - back:rim_rows - back + count] * taken[None, :, None]
    divisor = jnp.minimum(positions[:, None] + 1.0, window[None, :])
    return (total / divisor[:, :, None] - current).astype(jnp.bfloat16)

def one_sequence(tokens, input_gain, query_weight, latent_down, rotary_down, pool_down, key_up, value_up, query_gain, key_gain, pool_weight, pool_scale, attention_gain, pool_gain, attention_out, pool_out):
    count = tokens.shape[0]
    source = tokens.astype(jnp.float32)
    normed = (source * rms_scale(source) * input_gain).astype(jnp.bfloat16)
    latent_rows = jnp.concatenate([jnp.dot(normed, latent_down, preferred_element_type=jnp.float32), jnp.dot(normed, rotary_down, preferred_element_type=jnp.float32)], axis=1).astype(jnp.bfloat16)
    query_raw = jnp.dot(normed, query_weight, preferred_element_type=jnp.float32).reshape(count, HEADS, QK_DIM)
    pool_input = jnp.dot(normed, pool_down, preferred_element_type=jnp.float32).astype(jnp.bfloat16)
    positions_int = jnp.arange(count, dtype=jnp.int32)
    positions = positions_int.astype(jnp.float32)
    queries = lax.optimization_barrier(head_vectors(query_raw, query_gain, positions)).astype(jnp.float32)
    keys, values = expand_keys(latent_rows, 0, key_up, value_up, key_gain)
    keys = lax.optimization_barrier(keys).astype(jnp.float32)
    values = lax.optimization_barrier(values).astype(jnp.float32)
    factor = 1.0 / math.sqrt(QK_DIM)
    qblock = math.gcd(count, 512)

    def attend_block(index):
        begin = index * qblock
        query_block = lax.dynamic_slice_in_dim(queries, begin, qblock, 0)
        scores = jnp.einsum('qhd,khd->hqk', query_block, keys) * factor
        query_pos = begin + jnp.arange(qblock, dtype=jnp.int32)
        visible = positions_int[None, None, :] <= query_pos[None, :, None]
        weights = jnp.where(visible, jnp.exp(scores), 0.0)
        rounded = lax.optimization_barrier(weights.astype(jnp.bfloat16)).astype(jnp.float32)
        numer = jnp.einsum('hqk,khd->qhd', rounded, values)
        denom = lax.optimization_barrier(jnp.sum(weights, axis=-1))
        return numer / jnp.transpose(denom)[:, :, None]
    attended = lax.map(attend_block, jnp.arange(count // qblock, dtype=jnp.int32))
    attended = attended.reshape(count, HEADS * VALUE_DIM)
    before = jnp.zeros((rim_rows, POOL_WIDTH), jnp.bfloat16)
    pooled_mean = pool_mix(pool_input, before, jnp.arange(GROUPS, dtype=jnp.int32), positions)
    pooled = jnp.einsum('rgc,gcd->rgd', pooled_mean.astype(jnp.float32), pool_weight.astype(jnp.float32))
    pooled = pooled.reshape(count, POOL_WIDTH) * pool_scale
    attention_mixed = (attended * rms_scale(attended) * attention_gain).astype(jnp.bfloat16)
    pool_mixed = (pooled * rms_scale(pooled) * pool_gain).astype(jnp.bfloat16)
    head_cols = HEADS * VALUE_DIM // HEAD_BLOCKS
    pool_cols = POOL_WIDTH // HEAD_BLOCKS
    total = jnp.zeros((count, D), jnp.float32)
    for member in range(HEAD_BLOCKS):
        term = jnp.dot(attention_mixed[:, member * head_cols:(member + 1) * head_cols], attention_out[member * head_cols:(member + 1) * head_cols], preferred_element_type=jnp.float32)
        term = term + jnp.dot(pool_mixed[:, member * pool_cols:(member + 1) * pool_cols], pool_out[member * pool_cols:(member + 1) * pool_cols], preferred_element_type=jnp.float32)
        total = total + lax.optimization_barrier(term.astype(jnp.bfloat16)).astype(jnp.float32)
    return total.astype(jnp.bfloat16)

def reference(tokens, input_gain, query_weight, latent_down, rotary_down, pool_down, key_up, value_up, query_gain, key_gain, pool_weight, pool_scale, attention_gain, pool_gain, attention_out, pool_out):
    results = []
    for sequence in range(SEQS):
        results.append(one_sequence(tokens[sequence], input_gain, query_weight, latent_down, rotary_down, pool_down, key_up, value_up, query_gain, key_gain, pool_weight, pool_scale, attention_gain, pool_gain, attention_out, pool_out))
    return jnp.stack(results)
```

```python
import math

import jax
import jax.numpy as jnp
import numpy as np
from jax import lax
from jax.experimental import pallas as pl
from jax.experimental.pallas import tpu as pltpu
from jax.sharding import PartitionSpec as P

HEADS = 8
NOPE_DIM = 64
ROPE_DIM = 32
VALUE_DIM = 128
KV_LATENT = 256
GROUP_DIM = 64
QK_DIM = 96
D = 2048
BLOCKS = 16
BLOCK = 512
CHIPS = 4
ROWS = 64
LANES = 128
QROWS = CHIPS * ROWS
KEYS = BLOCKS * 2 * ROWS
HALO = 16
LAT = 384

EPS = 1e-06
THETA = 10000.0
SAME_CORE = [[0, 2, 4, 6], [1, 3, 5, 7]]
F32 = jnp.float32
BF16 = jnp.bfloat16


def angle_tables():
    half = ROPE_DIM // 2
    freq = np.zeros(LANES)
    inv = 1.0 / THETA ** (np.arange(half, dtype=np.float64) / half)
    freq[NOPE_DIM : NOPE_DIM + half] = inv
    freq[NOPE_DIM + half : QK_DIM] = inv
    inside = np.arange(BLOCK)[:, None] * freq[None, :]
    starts = (np.arange(BLOCKS) * BLOCK)[:, None] * freq[None, :]
    inside = np.stack([np.cos(inside), np.sin(inside)]).astype(np.float32)
    starts = np.stack([np.cos(starts), np.sin(starts)]).astype(np.float32)
    return inside.reshape(2, CHIPS, 2, ROWS, LANES), starts


def among_chips(array):
    return lax.all_to_all(array, "tp", 0, 0, axis_index_groups=SAME_CORE, tiled=True)


def to_partner(array):
    return lax.ppermute(array, "tp", [(i, i ^ 1) for i in range(2 * CHIPS)])


def whole(kernel, out_shape, *args, smem=1, scratch=(), name=None):
    single = not isinstance(out_shape, (list, tuple))
    outs = [out_shape] if single else list(out_shape)
    specs = [pl.BlockSpec(memory_space=pltpu.SMEM)] * smem
    specs += [pl.BlockSpec(memory_space=pltpu.VMEM)] * (len(args) - smem)
    out_specs = [pl.BlockSpec(memory_space=pltpu.VMEM)] * len(outs)
    return pl.pallas_call(
        kernel,
        out_shape=out_shape,
        in_specs=specs,
        out_specs=out_specs[0] if single else out_specs,
        scratch_shapes=list(scratch),
        compiler_params=pltpu.CompilerParams(vmem_limit_bytes=56 * 1024 * 1024),
        name=name,
    )(*args)


def dot(a, b, dims=((1,), (0,)), precision=None):
    return lax.dot_general(
        a, b, (dims, ((), ())), preferred_element_type=F32, precision=precision
    )


def turn(vectors, cosine, sine):
    lane = lax.broadcasted_iota(jnp.int32, vectors.shape, vectors.ndim - 1)
    half = ROPE_DIM // 2
    ahead = pltpu.roll(vectors, LANES - half, vectors.ndim - 1)
    behind = pltpu.roll(vectors, half, vectors.ndim - 1)
    return vectors * cosine + jnp.where(lane < NOPE_DIM + half, -ahead, behind) * sine


def at_block(inside_cos, inside_sin, start_cos, start_sin):
    cosine = start_cos * inside_cos - start_sin * inside_sin
    sine = start_sin * inside_cos + start_cos * inside_sin
    return cosine, sine


def norm_kernel(tokens, gain, latent_down, rotary_down, normed_out, latent_out):
    source = tokens[0].astype(F32)
    scale = lax.rsqrt(jnp.mean(source * source, axis=-1, keepdims=True) + EPS)
    normed = (source * scale * gain[...]).astype(BF16)
    for chip in range(CHIPS):
        normed_out[chip] = normed
    latent_out[:, :KV_LATENT] = dot(normed, latent_down[...]).astype(BF16)
    latent_out[:, KV_LATENT:] = dot(normed, rotary_down[...]).astype(BF16)


def project_kernel(coords, rows, own, other, gain, inside, starts, query_out, pool_out):
    z, p = coords[0], coords[2]
    piece = rows[...].reshape(QROWS, D)
    start_cos = starts[0, pl.ds(z, 1), :]
    start_sin = starts[1, pl.ds(z, 1), :]
    inside_cos = jnp.concatenate([inside[0, c, p] for c in range(CHIPS)], axis=0)
    inside_sin = jnp.concatenate([inside[1, c, p] for c in range(CHIPS)], axis=0)
    cosine, sine = at_block(inside_cos, inside_sin, start_cos, start_sin)
    for weights, slot in ((own, p), (other, 1 - p)):
        both = dot(piece, weights[...])
        raw = both[:, :LANES]
        square = jnp.sum(raw * raw, axis=-1, keepdims=True) * (1.0 / QK_DIM)
        normal = raw * lax.rsqrt(square + EPS) * gain[...]
        queries = turn(normal, cosine, sine).astype(BF16)
        for chip in range(CHIPS):
            query_out[chip, slot] = queries
        pool_out[slot] = both[:, LANES:].astype(BF16)


def expand_kernel(coords, own, other, key_up, gain, inside, starts, keys_out, latent_out):
    z, x, p = coords[0], coords[1], coords[2]
    lane = lax.broadcasted_iota(jnp.int32, (1, LANES), 1)
    plain_gain = jnp.where(lane < NOPE_DIM, gain[...], 0.0)
    rotary_gain = jnp.where(lane < NOPE_DIM, 0.0, gain[...])

    def one(block, carry):
        start_cos = starts[0, pl.ds(block, 1), :]
        start_sin = starts[1, pl.ds(block, 1), :]
        for rows, slot in ((own, p), (other, 1 - p)):
            at = block * 2 * ROWS + slot * ROWS
            at = pl.multiple_of(at, ROWS)
            packed = rows[block].astype(F32)
            latent = packed[:, :KV_LATENT]
            scale = lax.rsqrt(jnp.mean(latent * latent, axis=-1, keepdims=True) + EPS)
            normed = (latent * scale).astype(BF16)
            latent_out[pl.ds(at, ROWS), :] = normed
            shared = packed[:, KV_LATENT:]
            shared_square = jnp.sum(shared * shared, axis=-1, keepdims=True)
            cosine, sine = at_block(inside[0, x, slot], inside[1, x, slot], start_cos, start_sin)
            turned = turn(shared * rotary_gain, cosine, sine)
            plain = dot(normed, key_up[...])
            for head in range(HEADS):
                part = plain[:, head * LANES : (head + 1) * LANES]
                square = jnp.sum(part * part, axis=-1, keepdims=True) + shared_square
                factor = lax.rsqrt(square * (1.0 / QK_DIM) + EPS)
                keys_out[head, pl.ds(at, ROWS), :] = (
                    (part * plain_gain + turned) * factor
                ).astype(BF16)
        return carry

    lax.fori_loop(0, jnp.minimum((z // 2) * 2 + 2, BLOCKS), one, 0)


def attend_kernel(coords, queries, keys, latents, value_up, out, sums, totals):
    z, x, p = coords[0], coords[1], coords[2]
    factor = math.log2(math.e) / math.sqrt(QK_DIM)
    wide = 4 * ROWS

    def chunk(at, mask, first):
        at = pl.multiple_of(at, wide)
        latent = latents[pl.ds(at, wide), :]
        for head in range(HEADS):
            scores = dot(queries[head], keys[head, pl.ds(at, wide), :], ((1,), (1,)))
            weights = jnp.exp2(scores * factor)
            if mask is not None:
                weights = jnp.where(mask, weights, 0.0)
            part = weights[:, :LANES] + weights[:, LANES:]
            numer = dot(weights.astype(BF16), latent)
            if first:
                totals[head] = part
                sums[head] = numer
            else:
                totals[head] += part
                sums[head] += numer

    pair = z // 2
    row = lax.broadcasted_iota(jnp.int32, (QROWS, wide), 0)
    col = lax.broadcasted_iota(jnp.int32, (QROWS, wide), 1)
    query_pos = z * BLOCK + (row // ROWS) * (2 * ROWS) + p * ROWS + row % ROWS
    key_pos = (2 * pair + col // (2 * ROWS)) * BLOCK + x * (2 * ROWS) + col % (2 * ROWS)
    chunk(pair * wide, key_pos <= query_pos, True)

    def body(index, carry):
        chunk(index * wide, None, False)
        return carry

    lax.fori_loop(0, pair, body, 0)
    ones = jnp.ones((HALO, LANES), F32)
    line = lax.broadcasted_iota(jnp.int32, (HALO, QROWS), 0)
    for chip in range(CHIPS):
        tail = jnp.zeros((HALO, QROWS), F32)
        for slot in range(2):
            head = 2 * chip + slot
            values = value_up[:, head * VALUE_DIM : (head + 1) * VALUE_DIM]
            numer = dot(sums[head].astype(BF16), values)
            out[chip, :QROWS, slot * LANES : (slot + 1) * LANES] = numer.astype(BF16)
            denom = dot(ones, totals[head], ((1,), (1,)), lax.Precision.HIGHEST)
            high = denom.astype(BF16).astype(F32)
            tail = jnp.where(line == 2 * slot, high, tail)
            tail = jnp.where(line == 2 * slot + 1, denom - high, tail)
        out[chip, QROWS:, :] = tail.astype(BF16)


def pool_kernel(coords, pool_rows, halo, first_halo, weights, own, other, pooled_out, squares_out):
    z, p = coords[0], coords[2]
    lane = lax.broadcasted_iota(jnp.int32, (1, LANES), 1)
    row = lax.broadcasted_iota(jnp.int32, (ROWS, 1), 0)
    squares = jnp.zeros((QROWS, LANES), F32)
    for slot in range(2):
        scale = jnp.where(p == slot, own[0:1, :], other[0:1, :])
        small, large = (2, 4) if slot == 0 else (8, 16)
        window = jnp.where(lane < GROUP_DIM, small, large).astype(F32)
        means = []
        for chip in range(CHIPS):
            current = pool_rows[slot, chip * ROWS : (chip + 1) * ROWS, :].astype(F32)
            index = jnp.where(p == 1, chip, max(chip - 1, 0))
            before = halo[slot, index].astype(F32)
            if chip == 0:
                before = jnp.where(p == 1, before, first_halo[slot].astype(F32))
            total = jnp.concatenate([before, current], axis=0)
            reach = 1
            while reach < small:
                total = total + pltpu.roll(total, reach, 0)
                reach *= 2
            longer = total + pltpu.roll(total, reach, 0)
            total = jnp.where(lane < GROUP_DIM, total, longer)[HALO:]
            position = (z * BLOCK + chip * 2 * ROWS + p * ROWS + row).astype(F32)
            divisor = jnp.minimum(position + 1.0, window)
            means.append((total / divisor - current).astype(BF16))
        pooled = dot(jnp.concatenate(means, axis=0), weights[slot]) * scale
        pooled_out[slot] = pooled
        squares = squares + pooled * pooled
    squares_out[...] = squares


def join_kernel(parts, pool_squares, attended_out, squares_out):
    tail = jnp.zeros((HALO, QROWS), F32)
    for chip in range(CHIPS):
        tail = tail + parts[chip, QROWS:, :].astype(F32)
    columns = jnp.transpose(tail)
    squares = jnp.zeros((QROWS, LANES), F32)
    for slot in range(2):
        numer = jnp.zeros((QROWS, LANES), F32)
        for chip in range(CHIPS):
            numer = numer + parts[chip, :QROWS, slot * LANES : (slot + 1) * LANES].astype(F32)
        denom = columns[:, 2 * slot : 2 * slot + 1] + columns[:, 2 * slot + 1 : 2 * slot + 2]
        attended = numer / denom
        attended_out[slot] = attended
        squares = squares + attended * attended
    ones = jnp.ones((8, LANES), F32)
    exact = lax.Precision.HIGHEST
    line = lax.broadcasted_iota(jnp.int32, (8, QROWS), 0)
    mine = dot(ones, squares, ((1,), (1,)), exact)
    pools = dot(ones, pool_squares[...], ((1,), (1,)), exact)
    for chip in range(CHIPS):
        squares_out[chip] = jnp.where(line < 4, mine, pools)


def mix_kernel(
    coords, attended, pooled, squares, own_gain, other_gain, own_out, other_out, partial_out
):
    p = coords[2]
    total = jnp.transpose(squares[0] + squares[1] + squares[2] + squares[3])
    attention_factor = lax.rsqrt(total[:, 0:1] * (1.0 / (HEADS * VALUE_DIM)) + EPS)
    pool_factor = lax.rsqrt(total[:, 4:5] * (1.0 / (HEADS * VALUE_DIM)) + EPS)
    sides = []
    for gain, slot in ((own_gain, p), (other_gain, 1 - p)):
        sides.append(
            jnp.concatenate(
                [
                    (attended[slot] * attention_factor * gain[1:2, :]).astype(BF16),
                    (pooled[slot] * pool_factor * gain[2:3, :]).astype(BF16),
                ],
                axis=1,
            )
        )
    step = 512
    for at in range(0, D, step):
        both = dot(sides[0], own_out[:, at : at + step])
        both = both + dot(sides[1], other_out[:, at : at + step])
        partial_out[:, :, at : at + step] = both.astype(BF16).reshape(CHIPS, ROWS, step)


def sum_kernel(parts, out):
    total = parts[0].astype(F32) + parts[1].astype(F32)
    total = total + parts[2].astype(F32) + parts[3].astype(F32)
    out[0] = total.astype(BF16)


def local(
    tokens,
    input_gain,
    query_weight,
    latent_down,
    rotary_down,
    pool_down,
    key_up,
    value_up,
    query_gain,
    key_gain,
    pool_weight,
    pool_scale,
    attention_gain,
    pool_gain,
    attention_out,
    pool_out,
):
    member = lax.axis_index("tp")
    z = lax.axis_index("sp")
    x = member // 2
    coords = jnp.stack([z, x, member % 2]).astype(jnp.int32)
    inside, starts = (jnp.asarray(t) for t in angle_tables())
    pad = LANES - QK_DIM

    own_down = jnp.concatenate(
        [query_weight, jnp.zeros((D, pad), BF16), pool_down], axis=1
    )
    other_down = to_partner(own_down)
    rotary_wide = jnp.pad(rotary_down, ((0, 0), (NOPE_DIM, pad)))
    normed, latent_rows = whole(
        norm_kernel,
        (
            jax.ShapeDtypeStruct((CHIPS, ROWS, D), BF16),
            jax.ShapeDtypeStruct((ROWS, LAT), BF16),
        ),
        tokens,
        input_gain[None],
        latent_down,
        rotary_wide,
        smem=0,
        name="norm",
    )
    rows = among_chips(normed)
    own_latents = lax.all_gather(latent_rows, "sp", axis=0, tiled=False)
    other_latents = to_partner(own_latents)

    queries, pool_rows = whole(
        project_kernel,
        (
            jax.ShapeDtypeStruct((CHIPS, 2, QROWS, LANES), BF16),
            jax.ShapeDtypeStruct((2, QROWS, LANES), BF16),
        ),
        coords,
        rows,
        own_down,
        other_down,
        jnp.pad(query_gain, (0, pad))[None],
        inside,
        starts,
        name="project",
    )
    queries = among_chips(queries).reshape(HEADS, QROWS, LANES)

    key_wide = jnp.pad(
        key_up.reshape(KV_LATENT, HEADS, NOPE_DIM), ((0, 0), (0, 0), (0, LANES - NOPE_DIM))
    ).reshape(KV_LATENT, HEADS * LANES)
    keys, latents = whole(
        expand_kernel,
        (
            jax.ShapeDtypeStruct((HEADS, KEYS, LANES), BF16),
            jax.ShapeDtypeStruct((KEYS, KV_LATENT), BF16),
        ),
        coords,
        own_latents,
        other_latents,
        key_wide,
        jnp.pad(key_gain, (0, pad))[None],
        inside,
        starts,
        name="expand",
    )
    numer = whole(
        attend_kernel,
        jax.ShapeDtypeStruct((CHIPS, QROWS + HALO, 2 * LANES), BF16),
        coords,
        queries,
        keys,
        latents,
        value_up,
        scratch=(
            pltpu.VMEM((HEADS, QROWS, KV_LATENT), F32),
            pltpu.VMEM((HEADS, QROWS, LANES), F32),
        ),
        name="attend",
    )
    parts = among_chips(numer)

    tails = pool_rows.reshape(2, CHIPS, ROWS, LANES)[:, :, ROWS - HALO :]
    halo = to_partner(tails)
    width = 2 * CHIPS
    steps = [
        (block * width + 2 * chip + 1, (block + 1) * width + 2 * chip)
        for block in range(BLOCKS - 1)
        for chip in range(CHIPS)
    ]
    first_halo = lax.ppermute(tails[:, CHIPS - 1], ("sp", "tp"), steps)
    own_gain = jnp.stack([pool_scale, attention_gain, pool_gain])
    other_gain = to_partner(own_gain)
    own_out = jnp.concatenate([attention_out, pool_out], axis=0)
    other_out = to_partner(own_out)
    maps = lax.dynamic_slice_in_dim(pool_weight, x * 4, 4, 0).reshape(2, 2, GROUP_DIM, GROUP_DIM)
    same = jnp.eye(2, dtype=BF16)[None, :, None, :, None]
    maps = (maps[:, :, :, None, :] * same).reshape(2, LANES, LANES)
    pooled, pool_squares = whole(
        pool_kernel,
        (
            jax.ShapeDtypeStruct((2, QROWS, LANES), F32),
            jax.ShapeDtypeStruct((QROWS, LANES), F32),
        ),
        coords,
        pool_rows,
        halo,
        first_halo,
        maps,
        own_gain,
        other_gain,
        name="pool",
    )
    attended, squares = whole(
        join_kernel,
        (
            jax.ShapeDtypeStruct((2, QROWS, LANES), F32),
            jax.ShapeDtypeStruct((CHIPS, 8, QROWS), F32),
        ),
        parts,
        pool_squares,
        smem=0,
        name="join",
    )
    squares = among_chips(squares)
    partial = whole(
        mix_kernel,
        jax.ShapeDtypeStruct((CHIPS, ROWS, D), BF16),
        coords,
        attended,
        pooled,
        squares,
        own_gain,
        other_gain,
        own_out,
        other_out,
        name="mix",
    )
    return whole(
        sum_kernel, jax.ShapeDtypeStruct((1, ROWS, D), BF16), among_chips(partial), smem=0, name="sum"
    )


def solution(mesh):
    placed = (
        P("fs", ("sp", "tp"), None),
        P(),
        P(None, "tp"),
        P(),
        P(),
        P(None, "tp"),
        P(),
        P(),
        P(),
        P(),
        P(),
        P("tp"),
        P("tp"),
        P("tp"),
        P("tp", None),
        P("tp", None),
    )
    return jax.shard_map(
        local, mesh=mesh, in_specs=placed, out_specs=P("fs", ("sp", "tp"), None), check_vma=False
    )
```

```python
import math

import jax
import jax.numpy as jnp
import numpy as np
from jax import lax
from jax.experimental import pallas as pl
from jax.experimental.pallas import tpu as pltpu
from jax.sharding import PartitionSpec as P

HEADS = 8
NOPE_DIM = 64
ROPE_DIM = 32
VALUE_DIM = 128
KV_LATENT = 256
GROUP_DIM = 64
QK_DIM = 96
D = 2048
BLOCKS = 16
BLOCK = 512
CHIPS = 4
ROWS = 64
LANES = 128
QROWS = CHIPS * ROWS
KEYS = BLOCKS * 2 * ROWS
HALO = 16
LAT = 384

EPS = 1e-06
THETA = 10000.0
SAME_CORE = [[0, 2, 4, 6], [1, 3, 5, 7]]
F32 = jnp.float32
BF16 = jnp.bfloat16


def angle_tables():
    half = ROPE_DIM // 2
    freq = np.zeros(LANES)
    inv = 1.0 / THETA ** (np.arange(half, dtype=np.float64) / half)
    freq[NOPE_DIM : NOPE_DIM + half] = inv
    freq[NOPE_DIM + half : QK_DIM] = inv
    inside = np.arange(BLOCK)[:, None] * freq[None, :]
    starts = (np.arange(BLOCKS) * BLOCK)[:, None] * freq[None, :]
    inside = np.stack([np.cos(inside), np.sin(inside)]).astype(np.float32)
    starts = np.stack([np.cos(starts), np.sin(starts)]).astype(np.float32)
    return inside.reshape(2, CHIPS, 2, ROWS, LANES), starts


def among_chips(array):
    return lax.all_to_all(array, "tp", 0, 0, axis_index_groups=SAME_CORE, tiled=True)


def to_partner(array):
    return lax.ppermute(array, "tp", [(i, i ^ 1) for i in range(2 * CHIPS)])


MIB = 1024 * 1024
VECTOR = pl.BlockSpec(memory_space=pltpu.VMEM)
AWAY = pl.BlockSpec(memory_space=pltpu.HBM)
FLAT = 8192
AT_GAINS = 1536
AT_POOL = 2048
AT_OUT = 4096


def whole(kernel, out_shape, *args, specs=None, scratch=(), name=None, room=14):
    single = not isinstance(out_shape, (list, tuple))
    return pl.pallas_call(
        kernel,
        grid=() if specs is None else (1,),
        out_shape=out_shape,
        in_specs=[VECTOR] * len(args) if specs is None else specs,
        out_specs=VECTOR if single else [VECTOR] * len(out_shape),
        scratch_shapes=list(scratch),
        compiler_params=pltpu.CompilerParams(vmem_limit_bytes=room * MIB),
        name=name,
    )(*args)


def place():
    member = lax.axis_index("tp")
    return lax.axis_index("sp"), member // 2, member % 2


def shape(dims, dtype):
    return jax.ShapeDtypeStruct(dims, dtype)


def far(dims, dtype):
    return pltpu.HBM(dims, dtype)


def dot(a, b, dims=((1,), (0,)), precision=None):
    return lax.dot_general(
        a, b, (dims, ((), ())), preferred_element_type=F32, precision=precision
    )


def turn(vectors, cosine, sine):
    lane = lax.broadcasted_iota(jnp.int32, vectors.shape, vectors.ndim - 1)
    half = ROPE_DIM // 2
    ahead = pltpu.roll(vectors, LANES - half, vectors.ndim - 1)
    behind = pltpu.roll(vectors, half, vectors.ndim - 1)
    return vectors * cosine + jnp.where(lane < NOPE_DIM + half, -ahead, behind) * sine


def at_block(inside_cos, inside_sin, start_cos, start_sin):
    cosine = start_cos * inside_cos - start_sin * inside_sin
    sine = start_sin * inside_cos + start_cos * inside_sin
    return cosine, sine


def norm_kernel(tokens, gain, latent_down, rotary_down, normed_out, latent_out):
    source = tokens[0].astype(F32)
    scale = lax.rsqrt(jnp.mean(source * source, axis=-1, keepdims=True) + EPS)
    normed = (source * scale * gain[...]).astype(BF16)
    for chip in range(CHIPS):
        normed_out[chip] = normed
    latent_out[:, :KV_LATENT] = dot(normed, latent_down[...]).astype(BF16)
    above = jnp.zeros((NOPE_DIM, D), BF16)
    below = jnp.zeros((LANES - QK_DIM, D), BF16)
    rotary = jnp.concatenate([above, rotary_down[...], below], axis=0)
    latent_out[:, KV_LATENT:] = dot(normed, rotary, ((1,), (1,))).astype(BF16)


def bundle_kernel(query_t, pool_down, attention_out, pool_out, gains, after, flat):
    for at in range(D // LANES):
        lanes = slice(at * LANES, (at + 1) * LANES)
        flat[at * QK_DIM : (at + 1) * QK_DIM, :] = query_t[:, lanes]
        base = AT_OUT + at * 2 * LANES
        flat[base : base + LANES, :] = attention_out[:, lanes]
        flat[base + LANES : base + 2 * LANES, :] = pool_out[:, lanes]
    flat[AT_POOL:AT_OUT, :] = pool_down[...]
    rest = gains[...]
    rows = []
    for _ in range(3):
        piece = rest.astype(BF16)
        rest = rest - piece.astype(F32)
        rows.append(piece.astype(F32))
    rows.append(jnp.zeros((4, LANES), F32))
    flat[AT_GAINS : AT_GAINS + HALO, :] = jnp.concatenate(rows, axis=0).astype(BF16)


def unbundled_gains(rows):
    rows = rows.astype(F32)
    return rows[0:4] + rows[4:8] + rows[8:12]


def project_kernel(rows, own, other, gain, inside, starts, query_out, token_out):
    z, x, p = place()
    piece = rows[...].reshape(QROWS, D)
    start_cos = starts[0, pl.ds(z, 1), :]
    start_sin = starts[1, pl.ds(z, 1), :]
    inside_cos = jnp.concatenate([inside[0, c, p] for c in range(CHIPS)], axis=0)
    inside_sin = jnp.concatenate([inside[1, c, p] for c in range(CHIPS)], axis=0)
    cosine, sine = at_block(inside_cos, inside_sin, start_cos, start_sin)
    empty = jnp.zeros((LANES - QK_DIM, D), BF16)
    wide_gain = jnp.concatenate([gain[...], jnp.zeros((1, LANES - QK_DIM), F32)], axis=1)
    theirs = jnp.concatenate(
        [other[at * QK_DIM : (at + 1) * QK_DIM, :] for at in range(D // LANES)], axis=1
    )
    for weights, slot in ((own[...], p), (theirs, 1 - p)):
        raw = dot(piece, jnp.concatenate([weights, empty], axis=0), ((1,), (1,)))
        square = jnp.sum(raw * raw, axis=-1, keepdims=True) * (1.0 / QK_DIM)
        normal = raw * lax.rsqrt(square + EPS) * wide_gain
        queries = turn(normal, cosine, sine).astype(BF16)
        for chip in range(CHIPS):
            query_out[chip, slot] = queries
    token_out[...] = cosine[:8]


def pool_project_kernel(rows, own, other, after, pool_out, tails_out, last_out):
    z, x, p = place()
    piece = rows[...].reshape(QROWS, D)
    for weights, slot in ((own, p), (other, 1 - p)):
        result = dot(piece, weights[...]).astype(BF16)
        pool_out[slot] = result
        for chip in range(CHIPS):
            end = (chip + 1) * ROWS
            tails_out[slot, chip] = result[end - HALO : end]
        last_out[slot] = result[QROWS - HALO :]


def expand_kernel(own, other, key_up, gain, inside, starts, keys_out, latent_out):
    z, x, p = place()
    step = pl.program_id(0)

    @pl.when(step <= z // 2)
    def _():
        lane = lax.broadcasted_iota(jnp.int32, (1, LANES), 1)
        wide_gain = jnp.concatenate([gain[...], jnp.zeros((1, LANES - QK_DIM), F32)], axis=1)
        plain_gain = jnp.where(lane < NOPE_DIM, wide_gain, 0.0)
        rotary_gain = jnp.where(lane < NOPE_DIM, 0.0, wide_gain)
        pieces, cosines, sines = [], [], []
        for k in range(2):
            mine, theirs = own[k].astype(F32), other[k].astype(F32)
            pieces += [jnp.where(p == 0, mine, theirs), jnp.where(p == 0, theirs, mine)]
            start_cos = starts[0, pl.ds(2 * step + k, 1), :]
            start_sin = starts[1, pl.ds(2 * step + k, 1), :]
            for c in range(2):
                cosine, sine = at_block(inside[0, 0, c], inside[1, 0, c], start_cos, start_sin)
                cosines.append(cosine)
                sines.append(sine)
        packed = jnp.concatenate(pieces, axis=0)
        cosine = jnp.concatenate(cosines, axis=0)
        sine = jnp.concatenate(sines, axis=0)
        latent = packed[:, :KV_LATENT]
        scale = lax.rsqrt(jnp.mean(latent * latent, axis=-1, keepdims=True) + EPS)
        normed = (latent * scale).astype(BF16)
        latent_out[...] = normed
        shared = packed[:, KV_LATENT:]
        shared_square = jnp.sum(shared * shared, axis=-1, keepdims=True)
        turned = turn(shared * rotary_gain, cosine, sine)
        plain = dot(normed, key_up[...])
        for pair in range(HEADS // 2):
            group = plain[:, pair * LANES : (pair + 1) * LANES]
            for part, head in ((group, 2 * pair), (pltpu.roll(group, NOPE_DIM, 1), 2 * pair + 1)):
                part = jnp.where(lane < NOPE_DIM, part, 0.0)
                square = jnp.sum(part * part, axis=-1, keepdims=True) + shared_square
                factor = lax.rsqrt(square * (1.0 / QK_DIM) + EPS)
                keys_out[head] = ((part * plain_gain + turned) * factor).astype(BF16)


def attend_kernel(
    queries, keys_far, latents_far, value_far, out, keys, latents, value_up, sums, totals, arrived
):
    z, x, p = place()
    factor = math.log2(math.e) / math.sqrt(QK_DIM)
    wide = 4 * ROWS
    pair = z // 2

    def copies(index):
        at = pl.multiple_of(index * wide, wide)
        return (
            pltpu.make_async_copy(
                keys_far.at[:, pl.ds(at, wide), :],
                keys.at[:, pl.ds(at, wide), :],
                arrived.at[0, index],
            ),
            pltpu.make_async_copy(
                latents_far.at[pl.ds(at, wide), :],
                latents.at[pl.ds(at, wide), :],
                arrived.at[1, index],
            ),
        )

    def fetch(index, carry):
        for copy in copies(pair - index):
            copy.start()
        return carry

    lax.fori_loop(0, pair + 1, fetch, 0)
    value_copy = pltpu.make_async_copy(value_far, value_up, arrived.at[0, BLOCKS // 2])
    value_copy.start()

    def chunk(index, mask, first):
        at = pl.multiple_of(index * wide, wide)
        for copy in copies(index):
            copy.wait()
        latent = latents[pl.ds(at, wide), :]
        for head in range(HEADS):
            scores = dot(queries[head], keys[head, pl.ds(at, wide), :], ((1,), (1,)))
            weights = jnp.exp2(scores * factor)
            if mask is not None:
                weights = jnp.where(mask, weights, 0.0)
            part = weights[:, :LANES] + weights[:, LANES:]
            numer = dot(weights.astype(BF16), latent)
            if first:
                totals[head] = part
                sums[head] = numer
            else:
                totals[head] += part
                sums[head] += numer

    row = lax.broadcasted_iota(jnp.int32, (QROWS, wide), 0)
    col = lax.broadcasted_iota(jnp.int32, (QROWS, wide), 1)
    query_pos = z * BLOCK + (row // ROWS) * (2 * ROWS) + p * ROWS + row % ROWS
    key_pos = (2 * pair + col // (2 * ROWS)) * BLOCK + x * (2 * ROWS) + col % (2 * ROWS)
    chunk(pair, key_pos <= query_pos, True)

    def body(index, carry):
        chunk(pair - 1 - index, None, False)
        return carry

    lax.fori_loop(0, pair, body, 0)
    value_copy.wait()
    ones = jnp.ones((HALO, LANES), F32)
    line = lax.broadcasted_iota(jnp.int32, (HALO, QROWS), 0)
    for chip in range(CHIPS):
        tail = jnp.zeros((HALO, QROWS), F32)
        for slot in range(2):
            head = 2 * chip + slot
            values = value_up[:, head * VALUE_DIM : (head + 1) * VALUE_DIM]
            numer = dot(sums[head].astype(BF16), values)
            out[chip, :QROWS, slot * LANES : (slot + 1) * LANES] = numer.astype(BF16)
            denom = dot(ones, totals[head], ((1,), (1,)), lax.Precision.HIGHEST)
            high = denom.astype(BF16).astype(F32)
            tail = jnp.where(line == 2 * slot, high, tail)
            tail = jnp.where(line == 2 * slot + 1, denom - high, tail)
        out[chip, QROWS:, :] = tail.astype(BF16)


def pool_kernel(pool_rows, halo, first_halo, maps, own, other, pooled_out, squares_out):
    z, x, p = place()
    theirs = unbundled_gains(other[...])
    empty = jnp.zeros((GROUP_DIM, GROUP_DIM), F32)
    lane = lax.broadcasted_iota(jnp.int32, (1, LANES), 1)
    row = lax.broadcasted_iota(jnp.int32, (ROWS, 1), 0)
    squares = jnp.zeros((QROWS, LANES), F32)
    for slot in range(2):
        scale = jnp.where(p == slot, own[0:1, :], theirs[0:1, :])
        upper = jnp.concatenate([maps[4 * x + 2 * slot].astype(F32), empty], axis=1)
        lower = jnp.concatenate([empty, maps[4 * x + 2 * slot + 1].astype(F32)], axis=1)
        weights = jnp.concatenate([upper, lower], axis=0).astype(BF16)
        small, large = (2, 4) if slot == 0 else (8, 16)
        window = jnp.where(lane < GROUP_DIM, small, large).astype(F32)
        means = []
        for chip in range(CHIPS):
            current = pool_rows[slot, chip * ROWS : (chip + 1) * ROWS, :].astype(F32)
            index = jnp.where(p == 1, chip, max(chip - 1, 0))
            before = halo[slot, index].astype(F32)
            if chip == 0:
                before = jnp.where(p == 1, before, first_halo[slot].astype(F32))
            total = jnp.concatenate([before, current], axis=0)
            reach = 1
            while reach < small:
                total = total + pltpu.roll(total, reach, 0)
                reach *= 2
            longer = total + pltpu.roll(total, reach, 0)
            total = jnp.where(lane < GROUP_DIM, total, longer)[HALO:]
            position = (z * BLOCK + chip * 2 * ROWS + p * ROWS + row).astype(F32)
            divisor = jnp.minimum(position + 1.0, window)
            means.append((total / divisor - current).astype(BF16))
        pooled = dot(jnp.concatenate(means, axis=0), weights) * scale
        pooled_out[slot] = pooled
        squares = squares + pooled * pooled
    squares_out[...] = squares


def join_kernel(parts, pool_squares, attended_out, squares_out):
    tail = jnp.zeros((HALO, QROWS), F32)
    for chip in range(CHIPS):
        tail = tail + parts[chip, QROWS:, :].astype(F32)
    columns = jnp.transpose(tail)
    squares = jnp.zeros((QROWS, LANES), F32)
    for slot in range(2):
        numer = jnp.zeros((QROWS, LANES), F32)
        for chip in range(CHIPS):
            numer = numer + parts[chip, :QROWS, slot * LANES : (slot + 1) * LANES].astype(F32)
        denom = columns[:, 2 * slot : 2 * slot + 1] + columns[:, 2 * slot + 1 : 2 * slot + 2]
        attended = numer / denom
        attended_out[slot] = attended
        squares = squares + attended * attended
    ones = jnp.ones((8, LANES), F32)
    exact = lax.Precision.HIGHEST
    line = lax.broadcasted_iota(jnp.int32, (8, QROWS), 0)
    mine = dot(ones, squares, ((1,), (1,)), exact)
    pools = dot(ones, pool_squares[...], ((1,), (1,)), exact)
    for chip in range(CHIPS):
        squares_out[chip] = jnp.where(line < 4, mine, pools)


def mix_kernel(
    attended, pooled, squares, own_gain, other_gain, own_attention, own_pool, other_out, partial_out
):
    z, x, p = place()
    total = jnp.transpose(squares[0] + squares[1] + squares[2] + squares[3])
    attention_factor = lax.rsqrt(total[:, 0:1] * (1.0 / (HEADS * VALUE_DIM)) + EPS)
    pool_factor = lax.rsqrt(total[:, 4:5] * (1.0 / (HEADS * VALUE_DIM)) + EPS)
    sides = []
    for gain, slot in ((own_gain[...], p), (unbundled_gains(other_gain[...]), 1 - p)):
        sides.append((attended[slot] * attention_factor * gain[1:2, :]).astype(BF16))
        sides.append((pooled[slot] * pool_factor * gain[2:3, :]).astype(BF16))
    mine = jnp.concatenate(sides[:2], axis=1)
    theirs = jnp.concatenate(sides[2:], axis=1)
    step = 512
    for at in range(0, D, step):
        weights = jnp.concatenate(
            [own_attention[:, at : at + step], own_pool[:, at : at + step]], axis=0
        )
        far = jnp.concatenate(
            [
                other_out[base * 2 * LANES : (base + 1) * 2 * LANES, :]
                for base in range(at // LANES, (at + step) // LANES)
            ],
            axis=1,
        )
        both = dot(mine, weights) + dot(theirs, far)
        partial_out[:, :, at : at + step] = both.astype(BF16).reshape(CHIPS, ROWS, step)


def sum_kernel(parts, out):
    total = parts[0].astype(F32) + parts[1].astype(F32)
    total = total + parts[2].astype(F32) + parts[3].astype(F32)
    out[0] = total.astype(BF16)


def local(
    tokens,
    input_gain,
    query_weight,
    latent_down,
    rotary_down,
    pool_down,
    key_up,
    value_up,
    query_gain,
    key_gain,
    pool_weight,
    pool_scale,
    attention_gain,
    pool_gain,
    attention_out,
    pool_out,
):
    inside, starts = (jnp.asarray(t) for t in angle_tables())
    own_gain = jnp.stack([pool_scale, attention_gain, pool_gain, pool_gain])

    normed, latent_rows = whole(
        norm_kernel,
        (far((CHIPS, ROWS, D), BF16), shape((ROWS, LAT), BF16)),
        tokens,
        input_gain[None],
        latent_down,
        rotary_down.T,
        room=56,
        name="norm",
    )
    rows = among_chips(normed)
    query_t = query_weight.T
    other = to_partner(
        whole(
            bundle_kernel,
            shape((FLAT, LANES), BF16),
            query_t,
            pool_down,
            attention_out,
            pool_out,
            own_gain,
            normed,
            specs=[VECTOR] * 5 + [AWAY],
            room=56,
            name="bundle",
        )
    )
    own_latents = lax.all_gather(latent_rows, "sp", axis=0, tiled=False)
    other_latents = to_partner(own_latents)

    def part(length, at):
        return pl.BlockSpec((length, LANES), lambda i: (at // length, 0))

    queries, token = whole(
        project_kernel,
        (far((CHIPS, 2, QROWS, LANES), BF16), shape((8, LANES), F32)),
        rows,
        query_t,
        other,
        query_gain[None],
        inside,
        starts,
        specs=[VECTOR, VECTOR, part(AT_GAINS, 0), VECTOR, VECTOR, VECTOR],
        name="project",
    )
    queries = among_chips(queries).reshape(HEADS, QROWS, LANES)

    def chip():
        return lax.axis_index("tp") // 2

    def up_to(step):
        return jnp.minimum(step, lax.axis_index("sp") // 2)

    keys, latents = pl.pallas_call(
        expand_kernel,
        grid=(BLOCKS // 2,),
        out_shape=(far((HEADS, KEYS, LANES), BF16), far((KEYS, KV_LATENT), BF16)),
        in_specs=[
            pl.BlockSpec((2, ROWS, LAT), lambda i: (up_to(i), 0, 0)),
            pl.BlockSpec((2, ROWS, LAT), lambda i: (up_to(i), 0, 0)),
            pl.BlockSpec((KV_LATENT, HEADS * NOPE_DIM), lambda i: (0, 0)),
            pl.BlockSpec((1, QK_DIM), lambda i: (0, 0)),
            pl.BlockSpec((2, 1, 2, ROWS, LANES), lambda i: (0, chip(), 0, 0, 0)),
            pl.BlockSpec((2, BLOCKS, LANES), lambda i: (0, 0, 0)),
        ],
        out_specs=[
            pl.BlockSpec((HEADS, 4 * ROWS, LANES), lambda i: (0, up_to(i), 0)),
            pl.BlockSpec((4 * ROWS, KV_LATENT), lambda i: (up_to(i), 0)),
        ],
        compiler_params=pltpu.CompilerParams(vmem_limit_bytes=14 * MIB),
        name="expand",
    )(own_latents, other_latents, key_up, key_gain[None], inside, starts)

    pool_rows, tails, last_tails = whole(
        pool_project_kernel,
        (
            shape((2, QROWS, LANES), BF16),
            shape((2, CHIPS, HALO, LANES), BF16),
            shape((2, HALO, LANES), BF16),
        ),
        rows,
        pool_down,
        other,
        token,
        specs=[VECTOR, VECTOR, part(D, AT_POOL), VECTOR],
        name="pool_project",
    )
    halo = to_partner(tails)
    width = 2 * CHIPS
    steps = [
        (block * width + 2 * chip + 1, (block + 1) * width + 2 * chip)
        for block in range(BLOCKS - 1)
        for chip in range(CHIPS)
    ]
    first_halo = lax.ppermute(last_tails, ("sp", "tp"), steps)

    numer = whole(
        attend_kernel,
        far((CHIPS, QROWS + HALO, 2 * LANES), BF16),
        queries,
        keys,
        latents,
        value_up,
        specs=[VECTOR, AWAY, AWAY, AWAY],
        scratch=(
            pltpu.VMEM((HEADS, KEYS, LANES), BF16),
            pltpu.VMEM((KEYS, KV_LATENT), BF16),
            pltpu.VMEM((KV_LATENT, HEADS * VALUE_DIM), BF16),
            pltpu.VMEM((HEADS, QROWS, KV_LATENT), F32),
            pltpu.VMEM((HEADS, QROWS, LANES), F32),
            pltpu.SemaphoreType.DMA((2, BLOCKS // 2 + 1)),
        ),
        room=56,
        name="attend",
    )
    parts = among_chips(numer)

    pooled, pool_squares = whole(
        pool_kernel,
        (shape((2, QROWS, LANES), F32), shape((QROWS, LANES), F32)),
        pool_rows,
        halo,
        first_halo,
        pool_weight,
        own_gain,
        other,
        specs=[VECTOR] * 5 + [part(HALO, AT_GAINS)],
        name="pool",
    )
    attended, squares = whole(
        join_kernel,
        (shape((2, QROWS, LANES), F32), far((CHIPS, 8, QROWS), F32)),
        parts,
        pool_squares,
        name="join",
    )
    squares = among_chips(squares)
    partial = whole(
        mix_kernel,
        far((CHIPS, ROWS, D), BF16),
        attended,
        pooled,
        squares,
        own_gain,
        other,
        attention_out,
        pool_out,
        other,
        specs=[VECTOR] * 4 + [part(HALO, AT_GAINS), VECTOR, VECTOR, part(AT_OUT, AT_OUT)],
        name="mix",
    )
    return whole(sum_kernel, shape((1, ROWS, D), BF16), among_chips(partial), name="sum")


def solution(mesh):
    placed = (
        P("fs", ("sp", "tp"), None),
        P(),
        P(None, "tp"),
        P(),
        P(),
        P(None, "tp"),
        P(),
        P(),
        P(),
        P(),
        P(),
        P("tp"),
        P("tp"),
        P("tp"),
        P("tp", None),
        P("tp", None),
    )
    return jax.shard_map(
        local, mesh=mesh, in_specs=placed, out_specs=P("fs", ("sp", "tp"), None), check_vma=False
    )
```

```python
import math

import jax
import jax.numpy as jnp
import numpy as np
from jax import lax
from jax.experimental import pallas as pl
from jax.experimental.pallas import tpu as pltpu
from jax.sharding import PartitionSpec as P

HEADS = 8
NOPE_DIM = 64
ROPE_DIM = 32
VALUE_DIM = 128
KV_LATENT = 256
GROUP_DIM = 64
QK_DIM = 96
D = 2048
BLOCKS = 16
BLOCK = 512
CHIPS = 4
ROWS = 64
LANES = 128
QROWS = CHIPS * ROWS
KEYS = BLOCKS * 2 * ROWS
HALO = 16
PACK = ROWS + 8
QUAD = 4 * 2 * ROWS

EPS = 1e-06
THETA = 10000.0
SAME_CORE = [[0, 2, 4, 6], [1, 3, 5, 7]]
F32 = jnp.float32
BF16 = jnp.bfloat16


def angle_tables():
    half = ROPE_DIM // 2
    freq = np.zeros(LANES)
    inv = 1.0 / THETA ** (np.arange(half, dtype=np.float64) / half)
    freq[NOPE_DIM : NOPE_DIM + half] = inv
    freq[NOPE_DIM + half : QK_DIM] = inv
    inside = np.arange(BLOCK)[:, None] * freq[None, :]
    starts = (np.arange(BLOCKS) * BLOCK)[:, None] * freq[None, :]
    turned = (np.arange(BLOCK)[:, None] * inv[None, :]).reshape(CHIPS, 2 * ROWS, half)
    begins = (np.arange(BLOCKS) * BLOCK)[:, None] * inv[None, :]
    begins = np.broadcast_to(begins[:, :, None], (BLOCKS, half, LANES))
    tables = []
    for angle in (inside, starts, turned.transpose(0, 2, 1), begins):
        tables.append(np.stack([np.cos(angle), np.sin(angle)]).astype(np.float32))
    return tables


def among_chips(array):
    return lax.all_to_all(array, "tp", 0, 0, axis_index_groups=SAME_CORE, tiled=True)


def among_all(array):
    return lax.all_to_all(array, "tp", 0, 0, tiled=True)


def to_partner(array):
    return lax.ppermute(array, "tp", [(i, i ^ 1) for i in range(2 * CHIPS)])


MIB = 1024 * 1024
ROOM_PROJECT = 14
VECTOR = pl.BlockSpec(memory_space=pltpu.VMEM)
AWAY = pl.BlockSpec(memory_space=pltpu.HBM)


def whole(kernel, out_shape, *args, specs=None, scratch=(), room=14):
    single = not isinstance(out_shape, (list, tuple))
    return pl.pallas_call(
        kernel,
        grid=() if specs is None else (1,),
        out_shape=out_shape,
        in_specs=[VECTOR] * len(args) if specs is None else specs,
        out_specs=VECTOR if single else [VECTOR] * len(out_shape),
        scratch_shapes=list(scratch),
        compiler_params=pltpu.CompilerParams(vmem_limit_bytes=room * MIB),
    )(*args)


def place():
    member = lax.axis_index("tp")
    return lax.axis_index("sp"), member // 2, member % 2


def shape(dims, dtype):
    return jax.ShapeDtypeStruct(dims, dtype)


def far(dims, dtype):
    return pltpu.HBM(dims, dtype)


def dot(a, b, dims=((1,), (0,)), precision=None):
    return lax.dot_general(
        a, b, (dims, ((), ())), preferred_element_type=F32, precision=precision
    )


def turn(vectors, cosine, sine):
    lane = lax.broadcasted_iota(jnp.int32, vectors.shape, vectors.ndim - 1)
    half = ROPE_DIM // 2
    ahead = pltpu.roll(vectors, LANES - half, vectors.ndim - 1)
    behind = pltpu.roll(vectors, half, vectors.ndim - 1)
    return vectors * cosine + jnp.where(lane < NOPE_DIM + half, -ahead, behind) * sine


def at_block(inside_cos, inside_sin, start_cos, start_sin):
    cosine = start_cos * inside_cos - start_sin * inside_sin
    sine = start_sin * inside_cos + start_cos * inside_sin
    return cosine, sine


def norm_kernel(tokens, gain, latent_down, rotary_down, normed_out, latent_out):
    source = tokens[0].astype(F32)
    scale = lax.rsqrt(jnp.mean(source * source, axis=-1, keepdims=True) + EPS)
    normed = (source * scale * gain[...]).astype(BF16)
    for member in range(2 * CHIPS):
        normed_out[member] = normed
    latent = dot(normed, latent_down[...]).astype(BF16)
    rotary = dot(rotary_down[...], normed, ((1,), (1,)))
    packed = jnp.concatenate([rotary[at : at + 8] for at in range(0, ROPE_DIM, 8)], axis=1)
    latent_out[:ROWS] = latent
    latent_out[ROWS:] = packed.astype(BF16)


def out_bundle_kernel(attention_out, pool_out, gain_a, gain_p, both):
    both[:LANES, :] = attention_out[...]
    both[LANES : 2 * LANES, :] = pool_out[...]
    rest = jnp.concatenate([gain_a[...], gain_p[...]] * 2, axis=0)
    rows = []
    for _ in range(3):
        piece = rest.astype(BF16)
        rest = rest - piece.astype(F32)
        rows.append(piece.astype(F32))
    rows.append(jnp.zeros((4, LANES), F32))
    rows = jnp.concatenate(rows, axis=0)
    both[2 * LANES :, :] = jnp.concatenate([rows] * (D // LANES), axis=1).astype(BF16)


def project_kernel(rows, query_down, pool_down, gain, inside, starts, query_out, pool_out, tail_out):
    z, _, _ = place()
    piece = rows[...].reshape(BLOCK, D)
    start_cos = starts[0, pl.ds(z, 1), :]
    start_sin = starts[1, pl.ds(z, 1), :]
    cosine, sine = at_block(inside[0], inside[1], start_cos, start_sin)
    empty = jnp.zeros((LANES - QK_DIM, D), BF16)
    wide_gain = jnp.concatenate([gain[...], jnp.zeros((1, LANES - QK_DIM), F32)], axis=1)
    wide_gain = wide_gain * (math.log2(math.e) / math.sqrt(QK_DIM))
    raw = dot(piece, jnp.concatenate([query_down[...], empty], axis=0), ((1,), (1,)))
    square = jnp.sum(raw * raw, axis=-1, keepdims=True) * (1.0 / QK_DIM)
    normal = raw * lax.rsqrt(square + EPS) * wide_gain
    queries = turn(normal, cosine, sine).astype(BF16).reshape(CHIPS, 2, ROWS, LANES)
    for side in range(2):
        mine = queries[:, side].reshape(QROWS, LANES)
        for chip in range(CHIPS):
            query_out[2 * chip + side] = mine
    result = dot(piece, pool_down[...]).astype(BF16)
    pool_out[...] = result
    tail_out[...] = result[BLOCK - HALO :]


def expand_kernel(own, other, key_up, gain, inside, starts, keys_out, latent_out, key_up_t):
    z, _, p = place()
    step = pl.program_id(0)

    @pl.when(step == 0)
    def _():
        key_up_t[...] = jnp.transpose(key_up[...].astype(F32)).astype(BF16)

    @pl.when(step <= z // 4)
    def _():
        wide_gain = jnp.concatenate([gain[...], jnp.zeros((1, LANES - QK_DIM), F32)], axis=1)
        wide_gain = jnp.broadcast_to(wide_gain * math.sqrt(QK_DIM), (8, LANES))
        column = jnp.transpose(wide_gain)[:, 0:1]
        half = ROPE_DIM // 2
        latents, rotaries, cosines, sines = [], [], [], []
        for k in range(4):
            mine, theirs = own[k].astype(F32), other[k].astype(F32)
            for side in (jnp.where(p == 0, mine, theirs), jnp.where(p == 0, theirs, mine)):
                latents.append(side[:ROWS])
                rotaries.append(
                    jnp.concatenate(
                        [side[ROWS:, at : at + ROWS] for at in range(0, KV_LATENT, ROWS)], axis=0
                    )
                )
            cosine, sine = at_block(inside[0, 0], inside[1, 0], starts[0, k], starts[1, k])
            cosines.append(cosine)
            sines.append(sine)
        latent = jnp.concatenate(latents, axis=0)
        rotary = jnp.concatenate(rotaries, axis=1)
        cosine = jnp.concatenate(cosines, axis=1)
        sine = jnp.concatenate(sines, axis=1)
        scale = lax.rsqrt(jnp.mean(latent * latent, axis=-1, keepdims=True) + EPS)
        normed = (latent * scale).astype(BF16)
        latent_out[...] = normed
        shared = jnp.sum(rotary * rotary, axis=0, keepdims=True) + QK_DIM * EPS
        ahead = rotary[:half] * column[NOPE_DIM : NOPE_DIM + half]
        behind = rotary[half:] * column[NOPE_DIM + half : QK_DIM]
        turned = jnp.concatenate(
            [ahead * cosine - behind * sine, behind * cosine + ahead * sine], axis=0
        )
        plain_gain = jnp.broadcast_to(column[:NOPE_DIM], (NOPE_DIM, QUAD))
        for head in range(HEADS):
            rows = key_up_t[head * NOPE_DIM : (head + 1) * NOPE_DIM, :]
            part = dot(rows, normed, ((1,), (1,)))
            factor = lax.rsqrt(jnp.sum(part * part, axis=0, keepdims=True) + shared)
            keys_out[head, :NOPE_DIM, :] = (part * plain_gain * factor).astype(BF16)
            keys_out[head, NOPE_DIM:, :] = (turned * factor).astype(BF16)


def attend_kernel(
    queries, keys_far, latents_far, value_far, out, keys, latents, value_up, sums, totals, arrived
):
    z, x, p = place()
    wide = QUAD
    pair = z // 4

    def copies(index):
        at = pl.multiple_of(index * wide, wide)
        return (
            pltpu.make_async_copy(
                keys_far.at[:, :, pl.ds(at, wide)],
                keys.at[:, :, pl.ds(at, wide)],
                arrived.at[0, index],
            ),
            pltpu.make_async_copy(
                latents_far.at[pl.ds(at, wide), :],
                latents.at[pl.ds(at, wide), :],
                arrived.at[1, index],
            ),
        )

    def fetch(index, carry):
        for copy in copies(pair - index):
            copy.start()
        return carry

    lax.fori_loop(0, pair + 1, fetch, 0)
    value_copy = pltpu.make_async_copy(value_far, value_up, arrived.at[0, BLOCKS // 4])
    value_copy.start()

    def chunk(index, mask, first):
        at = pl.multiple_of(index * wide, wide)
        for copy in copies(index):
            copy.wait()
        latent = latents[pl.ds(at, wide), :]
        for head in range(HEADS):
            scores = dot(queries[head, :, :QK_DIM], keys[head, :, pl.ds(at, wide)])
            weights = jnp.exp2(scores)
            if mask is not None:
                weights = jnp.where(mask, weights, 0.0)
            part = weights[:, :LANES]
            for lanes in range(LANES, wide, LANES):
                part = part + weights[:, lanes : lanes + LANES]
            numer = dot(weights.astype(BF16), latent)
            if first:
                totals[head] = part
                sums[head] = numer
            else:
                totals[head] += part
                sums[head] += numer

    row = lax.broadcasted_iota(jnp.int32, (QROWS, wide), 0)
    col = lax.broadcasted_iota(jnp.int32, (QROWS, wide), 1)
    query_pos = z * BLOCK + (row // ROWS) * (2 * ROWS) + p * ROWS + row % ROWS
    key_pos = (4 * pair + col // (2 * ROWS)) * BLOCK + x * (2 * ROWS) + col % (2 * ROWS)
    chunk(pair, key_pos <= query_pos, True)

    def body(index, carry):
        chunk(pair - 1 - index, None, False)
        return carry

    lax.fori_loop(0, pair, body, 0)
    value_copy.wait()
    ones = jnp.ones((HALO, LANES), F32)
    line = lax.broadcasted_iota(jnp.int32, (HALO, QROWS), 0)
    for chip in range(CHIPS):
        tail = jnp.zeros((HALO, QROWS), F32)
        for slot in range(2):
            head = 2 * chip + slot
            values = value_up[:, head * VALUE_DIM : (head + 1) * VALUE_DIM]
            numer = dot(sums[head].astype(BF16), values)
            out[chip, :QROWS, slot * LANES : (slot + 1) * LANES] = numer.astype(BF16)
            denom = dot(ones, totals[head], ((1,), (1,)), lax.Precision.HIGHEST)
            high = denom.astype(BF16).astype(F32)
            tail = jnp.where(line == 2 * slot, high, tail)
            tail = jnp.where(line == 2 * slot + 1, denom - high, tail)
        out[chip, QROWS:, :] = tail.astype(BF16)


def pool_kernel(pool_rows, halo, maps, scale, keep_out, give_out):
    z, x, p = place()
    lane = lax.broadcasted_iota(jnp.int32, (1, LANES), 1)
    early = lane < GROUP_DIM
    current = pool_rows[...].astype(F32)
    two = jnp.concatenate([halo[...].astype(F32), current], axis=0)
    two = two + pltpu.roll(two, 1, 0)
    four = two + pltpu.roll(two, 2, 0)
    eight = four + pltpu.roll(four, 4, 0)
    sixteen = eight + pltpu.roll(eight, 8, 0)
    short = jnp.where(early, two, four)
    long = jnp.where(early, eight, sixteen)
    total = jnp.where(p == 0, short, long)[HALO:]
    window = jnp.where(early, 2, 4) * jnp.where(p == 0, 1, 4)
    row = lax.broadcasted_iota(jnp.int32, (BLOCK, 1), 0)
    divisor = jnp.minimum((z * BLOCK + row).astype(F32) + 1.0, window.astype(F32))
    means = (total / divisor - current).astype(BF16)
    empty = jnp.zeros((GROUP_DIM, GROUP_DIM), F32)
    upper = jnp.concatenate([maps[4 * x + 2 * p].astype(F32), empty], axis=1)
    lower = jnp.concatenate([empty, maps[4 * x + 2 * p + 1].astype(F32)], axis=1)
    weights = jnp.concatenate([upper, lower], axis=0).astype(BF16)
    pooled = (dot(means, weights) * scale[...]).reshape(CHIPS, 2, ROWS, LANES)
    even = pooled[:, 0].reshape(QROWS, LANES)
    odd = pooled[:, 1].reshape(QROWS, LANES)
    keep_out[...] = jnp.where(p == 0, even, odd)
    give_out[...] = jnp.where(p == 0, odd, even)


def join_kernel(parts, pool_own, pool_other, attended_out, squares_out):
    tail = jnp.zeros((HALO, QROWS), F32)
    for chip in range(CHIPS):
        tail = tail + parts[chip, QROWS:, :].astype(F32)
    columns = jnp.transpose(tail)
    squares = jnp.zeros((QROWS, LANES), F32)
    for slot in range(2):
        numer = jnp.zeros((QROWS, LANES), F32)
        for chip in range(CHIPS):
            numer = numer + parts[chip, :QROWS, slot * LANES : (slot + 1) * LANES].astype(F32)
        denom = columns[:, 2 * slot : 2 * slot + 1] + columns[:, 2 * slot + 1 : 2 * slot + 2]
        attended = numer / denom
        attended_out[slot] = attended
        squares = squares + attended * attended
    ones = jnp.ones((8, LANES), F32)
    exact = lax.Precision.HIGHEST
    line = lax.broadcasted_iota(jnp.int32, (8, QROWS), 0)
    mine = dot(ones, squares, ((1,), (1,)), exact)
    pooled = pool_own[...] * pool_own[...] + pool_other[...] * pool_other[...]
    pools = dot(ones, pooled, ((1,), (1,)), exact)
    for chip in range(CHIPS):
        squares_out[chip] = jnp.where(line < 4, mine, pools)


def mix_kernel(
    attended,
    pool_own,
    pool_other,
    squares,
    gain_a,
    gain_p,
    own_attention,
    own_pool,
    other_out,
    partial_out,
):
    _, _, p = place()
    total = jnp.transpose(squares[0] + squares[1] + squares[2] + squares[3])
    attention_factor = lax.rsqrt(total[:, 0:1] * (1.0 / (HEADS * VALUE_DIM)) + EPS)
    pool_factor = lax.rsqrt(total[:, 4:5] * (1.0 / (HEADS * VALUE_DIM)) + EPS)
    sides = []
    rows = other_out[2 * LANES :, :LANES].astype(F32)
    far = rows[0:4] + rows[4:8] + rows[8:12]
    for first, second, pooled, slot in (
        (gain_a[...], gain_p[...], pool_own, p),
        (far[0:1, :], far[1:2, :], pool_other, 1 - p),
    ):
        sides.append((attended[slot] * attention_factor * first).astype(BF16))
        sides.append((pooled[...] * pool_factor * second).astype(BF16))
    mine = jnp.concatenate(sides[:2], axis=1)
    theirs = jnp.concatenate(sides[2:], axis=1)
    step = 512
    for at in range(0, D, step):
        weights = jnp.concatenate(
            [own_attention[:, at : at + step], own_pool[:, at : at + step]], axis=0
        )
        both = dot(mine, weights) + dot(theirs, other_out[: 2 * LANES, at : at + step])
        partial_out[:, :, at : at + step] = both.astype(BF16).reshape(CHIPS, ROWS, step)


def sum_kernel(parts, out):
    total = parts[0].astype(F32) + parts[1].astype(F32)
    total = total + parts[2].astype(F32) + parts[3].astype(F32)
    out[0] = total.astype(BF16)


def local(
    tokens,
    input_gain,
    query_weight,
    latent_down,
    rotary_down,
    pool_down,
    key_up,
    value_up,
    query_gain,
    key_gain,
    pool_weight,
    pool_scale,
    attention_gain,
    pool_gain,
    attention_out,
    pool_out,
):
    inside, starts, turned, begins = (jnp.asarray(t) for t in angle_tables())

    def chip():
        return lax.axis_index("tp") // 2

    def up_to(step):
        return jnp.minimum(step, lax.axis_index("sp") // 4)

    normed, latent_rows = whole(
        norm_kernel,
        (far((2 * CHIPS, ROWS, D), BF16), far((PACK, KV_LATENT), BF16)),
        tokens,
        input_gain[None],
        latent_down,
        rotary_down.T,
        room=56,
    )
    rows = among_all(normed)
    own_latents = lax.all_gather(latent_rows, "sp", axis=0, tiled=False)
    other_latents = to_partner(own_latents)

    queries, pool_rows, tail = whole(
        project_kernel,
        (
            far((2 * CHIPS, QROWS, LANES), BF16),
            shape((BLOCK, LANES), BF16),
            shape((HALO, LANES), BF16),
        ),
        rows,
        query_weight.T,
        pool_down,
        query_gain[None],
        inside,
        starts,
        room=ROOM_PROJECT,
    )
    queries = among_all(queries)
    halo = lax.ppermute(tail, "sp", [(i, i + 1) for i in range(BLOCKS - 1)])

    latent_spec = pl.BlockSpec((4, PACK, KV_LATENT), lambda i: (up_to(i), 0, 0))
    expand = pl.pallas_call(
        expand_kernel,
        grid=(BLOCKS // 4,),
        out_shape=(far((HEADS, QK_DIM, KEYS), BF16), far((KEYS, KV_LATENT), BF16)),
        in_specs=[
            latent_spec,
            latent_spec,
            pl.BlockSpec((KV_LATENT, HEADS * NOPE_DIM), lambda i: (0, 0)),
            pl.BlockSpec((1, QK_DIM), lambda i: (0, 0)),
            pl.BlockSpec((2, 1, ROPE_DIM // 2, LANES), lambda i: (0, chip(), 0, 0)),
            pl.BlockSpec((2, 4, ROPE_DIM // 2, LANES), lambda i: (0, up_to(i), 0, 0)),
        ],
        out_specs=[
            pl.BlockSpec((HEADS, QK_DIM, QUAD), lambda i: (0, 0, up_to(i))),
            pl.BlockSpec((QUAD, KV_LATENT), lambda i: (up_to(i), 0)),
        ],
        scratch_shapes=[pltpu.VMEM((HEADS * NOPE_DIM, KV_LATENT), BF16)],
        compiler_params=pltpu.CompilerParams(vmem_limit_bytes=56 * MIB),
        name="expand",
    )
    keys, latents = expand(own_latents, other_latents, key_up, key_gain[None], turned, begins)

    numer = whole(
        attend_kernel,
        far((CHIPS, QROWS + HALO, 2 * LANES), BF16),
        queries,
        keys,
        latents,
        value_up,
        specs=[VECTOR, AWAY, AWAY, AWAY],
        scratch=(
            pltpu.VMEM((HEADS, QK_DIM, KEYS), BF16),
            pltpu.VMEM((KEYS, KV_LATENT), BF16),
            pltpu.VMEM((KV_LATENT, HEADS * VALUE_DIM), BF16),
            pltpu.VMEM((HEADS, QROWS, KV_LATENT), F32),
            pltpu.VMEM((HEADS, QROWS, LANES), F32),
            pltpu.SemaphoreType.DMA((2, BLOCKS // 4 + 1)),
        ),
        room=56,
    )
    parts = among_chips(numer)

    pool_own, pool_give = whole(
        pool_kernel,
        (shape((QROWS, LANES), F32), shape((QROWS, LANES), F32)),
        pool_rows,
        halo,
        pool_weight,
        pool_scale[None],
    )
    pool_other = to_partner(pool_give)
    other_out = to_partner(
        whole(
            out_bundle_kernel,
            shape((2 * LANES + HALO, D), BF16),
            attention_out,
            pool_out,
            attention_gain[None],
            pool_gain[None],
        ),
    )
    attended, squares = whole(
        join_kernel,
        (shape((2, QROWS, LANES), F32), far((CHIPS, 8, QROWS), F32)),
        parts,
        pool_own,
        pool_other,
    )
    squares = among_chips(squares)
    partial = whole(
        mix_kernel,
        far((CHIPS, ROWS, D), BF16),
        attended,
        pool_own,
        pool_other,
        squares,
        attention_gain[None],
        pool_gain[None],
        attention_out,
        pool_out,
        other_out,
    )
    return whole(sum_kernel, shape((1, ROWS, D), BF16), among_chips(partial))


def solution(mesh):
    placed = (
        P("fs", ("sp", "tp"), None),
        P(),
        P(None, "tp"),
        P(),
        P(),
        P(None, "tp"),
        P(),
        P(),
        P(),
        P(),
        P(),
        P("tp"),
        P("tp"),
        P("tp"),
        P("tp", None),
        P("tp", None),
    )

    return jax.shard_map(
        local, mesh=mesh, in_specs=placed, out_specs=P("fs", ("sp", "tp"), None), check_vma=False
    )
```

```python
import math

import jax
import jax.numpy as jnp
import numpy as np
from jax import lax
from jax.experimental import pallas as pl
from jax.experimental.pallas import tpu as pltpu
from jax.sharding import PartitionSpec as P

HEADS = 8
NOPE_DIM = 64
ROPE_DIM = 32
VALUE_DIM = 128
KV_LATENT = 256
GROUP_DIM = 64
QK_DIM = 96
D = 2048
BLOCKS = 16
BLOCK = 512
CHIPS = 4
ROWS = 64
LANES = 128
QROWS = CHIPS * ROWS
KEYS = BLOCKS * 2 * ROWS
HALO = 16
PACK = ROWS + 8
QUAD = 4 * 2 * ROWS

EPS = 1e-06
THETA = 10000.0
SAME_CORE = [[0, 2, 4, 6], [1, 3, 5, 7]]
F32 = jnp.float32
BF16 = jnp.bfloat16


def angle_tables():
    half = ROPE_DIM // 2
    freq = np.zeros(LANES)
    inv = 1.0 / THETA ** (np.arange(half, dtype=np.float64) / half)
    freq[NOPE_DIM : NOPE_DIM + half] = inv
    freq[NOPE_DIM + half : QK_DIM] = inv
    inside = np.arange(BLOCK)[:, None] * freq[None, :]
    starts = (np.arange(BLOCKS) * BLOCK)[:, None] * freq[None, :]
    turned = (np.arange(BLOCK)[:, None] * inv[None, :]).reshape(CHIPS, 2 * ROWS, half)
    begins = (np.arange(BLOCKS) * BLOCK)[:, None] * inv[None, :]
    begins = np.broadcast_to(begins[:, :, None], (BLOCKS, half, LANES))
    tables = []
    for angle in (inside, starts, turned.transpose(0, 2, 1), begins):
        tables.append(np.stack([np.cos(angle), np.sin(angle)]).astype(np.float32))
    return tables


def among_chips(array):
    return lax.all_to_all(array, "tp", 0, 0, axis_index_groups=SAME_CORE, tiled=True)


def among_all(array):
    return lax.all_to_all(array, "tp", 0, 0, tiled=True)


def to_partner(array):
    return lax.ppermute(array, "tp", [(i, i ^ 1) for i in range(2 * CHIPS)])


MIB = 1024 * 1024
ROOM_PROJECT = 52
VECTOR = pl.BlockSpec(memory_space=pltpu.VMEM)
AWAY = pl.BlockSpec(memory_space=pltpu.HBM)


def whole(kernel, out_shape, *args, specs=None, outs=None, scratch=(), room=14):
    single = not isinstance(out_shape, (list, tuple))
    return pl.pallas_call(
        kernel,
        grid=() if specs is None else (1,),
        out_shape=out_shape,
        in_specs=[VECTOR] * len(args) if specs is None else specs,
        out_specs=outs or (VECTOR if single else [VECTOR] * len(out_shape)),
        scratch_shapes=list(scratch),
        compiler_params=pltpu.CompilerParams(vmem_limit_bytes=room * MIB),
    )(*args)


def place():
    member = lax.axis_index("tp")
    return lax.axis_index("sp"), member // 2, member % 2


def shape(dims, dtype):
    return jax.ShapeDtypeStruct(dims, dtype)


def far(dims, dtype):
    return pltpu.HBM(dims, dtype)


def dot(a, b, dims=((1,), (0,)), precision=None):
    return lax.dot_general(
        a, b, (dims, ((), ())), preferred_element_type=F32, precision=precision
    )


def turn(vectors, cosine, sine):
    lane = lax.broadcasted_iota(jnp.int32, vectors.shape, vectors.ndim - 1)
    half = ROPE_DIM // 2
    ahead = pltpu.roll(vectors, LANES - half, vectors.ndim - 1)
    behind = pltpu.roll(vectors, half, vectors.ndim - 1)
    return vectors * cosine + jnp.where(lane < NOPE_DIM + half, -ahead, behind) * sine


def at_block(inside_cos, inside_sin, start_cos, start_sin):
    cosine = start_cos * inside_cos - start_sin * inside_sin
    sine = start_sin * inside_cos + start_cos * inside_sin
    return cosine, sine


def norm_kernel(
    tokens, gain, latent_down, rotary_down, query_gain, normed_out, latent_out, gain_out
):
    source = tokens[0].astype(F32)
    scale = lax.rsqrt(jnp.mean(source * source, axis=-1, keepdims=True) + EPS)
    normed = (source * scale * gain[...]).astype(BF16)
    for member in range(2 * CHIPS):
        normed_out[member] = normed
    rotary = dot(rotary_down[...], normed, ((1,), (1,)))
    packed = jnp.concatenate([rotary[at : at + 8] for at in range(0, ROPE_DIM, 8)], axis=1)
    latent_out[ROWS:] = packed.astype(BF16)
    wide = jnp.concatenate([query_gain[...], jnp.zeros((1, LANES - QK_DIM), F32)], axis=1)
    wide = wide * (math.log2(math.e) / math.sqrt(QK_DIM))
    gain_out[...] = jnp.broadcast_to(wide, (8, LANES))
    latent_out[:ROWS] = dot(normed, latent_down[...]).astype(BF16)


def out_bundle_kernel(attention_out, pool_out, gain_a, gain_p, both):
    both[:LANES, :] = attention_out[...]
    both[LANES : 2 * LANES, :] = pool_out[...]
    rest = jnp.concatenate([gain_a[...], gain_p[...]] * 2, axis=0)
    rows = []
    for _ in range(3):
        piece = rest.astype(BF16)
        rest = rest - piece.astype(F32)
        rows.append(piece.astype(F32))
    rows.append(jnp.zeros((4, LANES), F32))
    rows = jnp.concatenate(rows, axis=0)
    both[2 * LANES :, :] = jnp.concatenate([rows] * (D // LANES), axis=1).astype(BF16)


def project_kernel(
    rows_far,
    query_down,
    pool_down,
    gain,
    inside,
    starts,
    query_out,
    pool_out,
    tail_out,
    rows,
    arrived,
):
    z, _, _ = place()
    per = CHIPS
    copies = []
    for part in range(2):
        span = pl.ds(part * per, per)
        copies.append(
            pltpu.make_async_copy(rows_far.at[span], rows.at[span], arrived.at[part])
        )
        copies[-1].start()
    start_cos = starts[0, pl.ds(z, 1), :]
    start_sin = starts[1, pl.ds(z, 1), :]
    cosine, sine = at_block(inside[0], inside[1], start_cos, start_sin)
    empty = jnp.zeros((LANES - QK_DIM, D), BF16)
    query_wide = jnp.concatenate([query_down[...], empty], axis=0)
    half = per * ROWS
    for part in range(2):
        copies[part].wait()
        piece = rows[part * per : (part + 1) * per].reshape(half, D)
        raw = dot(piece, query_wide, ((1,), (1,)))
        square = jnp.sum(raw * raw, axis=-1, keepdims=True) * (1.0 / QK_DIM)
        normal = raw * lax.rsqrt(square + EPS) * gain[0:1, :]
        span = slice(part * half, (part + 1) * half)
        queries = turn(normal, cosine[span], sine[span]).astype(BF16)
        for member in range(per):
            mine = queries[member * ROWS : (member + 1) * ROWS]
            side, chip = member % 2, (part * per + member) // 2
            for target in range(CHIPS):
                query_out[2 * target + side, chip * ROWS : (chip + 1) * ROWS] = mine
        result = dot(piece, pool_down[...]).astype(BF16)
        pool_out[part * half : (part + 1) * half] = result
    tail_out[...] = result[half - HALO :]


def expand_kernel(own, other, key_up, gain, inside, starts, keys_out, latent_out, key_up_t):
    z, _, p = place()
    step = pl.program_id(0)

    @pl.when(step == 0)
    def _():
        key_up_t[...] = jnp.transpose(key_up[...].astype(F32)).astype(BF16)

    @pl.when(step <= z // 4)
    def _():
        wide_gain = jnp.concatenate([gain[...], jnp.zeros((1, LANES - QK_DIM), F32)], axis=1)
        wide_gain = jnp.broadcast_to(wide_gain * math.sqrt(QK_DIM), (8, LANES))
        column = jnp.transpose(wide_gain)[:, 0:1]
        half = ROPE_DIM // 2
        latents, rotaries, cosines, sines = [], [], [], []
        for k in range(4):
            mine, theirs = own[k].astype(F32), other[k].astype(F32)
            for side in (jnp.where(p == 0, mine, theirs), jnp.where(p == 0, theirs, mine)):
                latents.append(side[:ROWS])
                rotaries.append(
                    jnp.concatenate(
                        [side[ROWS:, at : at + ROWS] for at in range(0, KV_LATENT, ROWS)], axis=0
                    )
                )
            cosine, sine = at_block(inside[0, 0], inside[1, 0], starts[0, k], starts[1, k])
            cosines.append(cosine)
            sines.append(sine)
        latent = jnp.concatenate(latents, axis=0)
        rotary = jnp.concatenate(rotaries, axis=1)
        cosine = jnp.concatenate(cosines, axis=1)
        sine = jnp.concatenate(sines, axis=1)
        scale = lax.rsqrt(jnp.mean(latent * latent, axis=-1, keepdims=True) + EPS)
        normed = (latent * scale).astype(BF16)
        latent_out[...] = normed
        shared = jnp.sum(rotary * rotary, axis=0, keepdims=True) + QK_DIM * EPS
        ahead = rotary[:half] * column[NOPE_DIM : NOPE_DIM + half]
        behind = rotary[half:] * column[NOPE_DIM + half : QK_DIM]
        turned = jnp.concatenate(
            [ahead * cosine - behind * sine, behind * cosine + ahead * sine], axis=0
        )
        plain_gain = jnp.broadcast_to(column[:NOPE_DIM], (NOPE_DIM, QUAD))
        for head in range(HEADS):
            rows = key_up_t[head * NOPE_DIM : (head + 1) * NOPE_DIM, :]
            part = dot(rows, normed, ((1,), (1,)))
            factor = lax.rsqrt(jnp.sum(part * part, axis=0, keepdims=True) + shared)
            keys_out[head, :NOPE_DIM, :] = (part * plain_gain * factor).astype(BF16)
            keys_out[head, NOPE_DIM:, :] = (turned * factor).astype(BF16)


def attend_kernel(
    queries,
    keys_far,
    latents_far,
    value_far,
    out_far,
    out,
    keys,
    latents,
    value_up,
    sums,
    totals,
    arrived,
):
    z, x, p = place()
    wide = QUAD
    pair = z // 4

    def copies(index):
        at = pl.multiple_of(index * wide, wide)
        return (
            pltpu.make_async_copy(
                keys_far.at[:, :, pl.ds(at, wide)],
                keys.at[:, :, pl.ds(at, wide)],
                arrived.at[0, index],
            ),
            pltpu.make_async_copy(
                latents_far.at[pl.ds(at, wide), :],
                latents.at[pl.ds(at, wide), :],
                arrived.at[1, index],
            ),
        )

    def fetch(index, carry):
        for copy in copies(pair - index):
            copy.start()
        return carry

    lax.fori_loop(0, pair + 1, fetch, 0)
    value_copy = pltpu.make_async_copy(value_far, value_up, arrived.at[0, BLOCKS // 4])
    value_copy.start()

    def chunk(index, mask, first, width=QUAD):
        at = pl.multiple_of(index * wide, wide)
        for copy in copies(index):
            copy.wait()
        latent = latents[pl.ds(at, width), :]
        for head in range(HEADS):
            scores = dot(queries[head, :, :QK_DIM], keys[head, :, pl.ds(at, width)])
            weights = jnp.exp2(scores)
            if mask is not None:
                weights = jnp.where(mask, weights, 0.0)
            part = weights[:, :LANES]
            for lanes in range(LANES, width, LANES):
                part = part + weights[:, lanes : lanes + LANES]
            numer = dot(weights.astype(BF16), latent)
            if first:
                totals[head] = part
                sums[head] = numer
            else:
                totals[head] += part
                sums[head] += numer

    def last(width):
        row = lax.broadcasted_iota(jnp.int32, (QROWS, width), 0)
        col = lax.broadcasted_iota(jnp.int32, (QROWS, width), 1)
        query_pos = z * BLOCK + (row // ROWS) * (2 * ROWS) + p * ROWS + row % ROWS
        key_pos = (4 * pair + col // (2 * ROWS)) * BLOCK + x * (2 * ROWS) + col % (2 * ROWS)
        chunk(pair, key_pos <= query_pos, True, width)

    @pl.when(z % 4 < 2)
    def _():
        last(QUAD // 2)

    @pl.when(z % 4 >= 2)
    def _():
        last(QUAD)

    def body(index, carry):
        chunk(pair - 1 - index, None, False)
        return carry

    lax.fori_loop(0, pair, body, 0)
    value_copy.wait()
    sends = []
    ones = jnp.ones((HALO, LANES), F32)
    line = lax.broadcasted_iota(jnp.int32, (HALO, QROWS), 0)
    for chip in range(CHIPS):
        tail = jnp.zeros((HALO, QROWS), F32)
        for slot in range(2):
            head = 2 * chip + slot
            values = value_up[:, head * VALUE_DIM : (head + 1) * VALUE_DIM]
            numer = dot(sums[head].astype(BF16), values)
            out[chip, :QROWS, slot * LANES : (slot + 1) * LANES] = numer.astype(BF16)
            denom = dot(ones, totals[head], ((1,), (1,)), lax.Precision.HIGHEST)
            high = denom.astype(BF16).astype(F32)
            tail = jnp.where(line == 2 * slot, high, tail)
            tail = jnp.where(line == 2 * slot + 1, denom - high, tail)
        out[chip, QROWS:, :] = tail.astype(BF16)
        sends.append(pltpu.make_async_copy(out.at[chip], out_far.at[chip], arrived.at[2, chip]))
        sends[-1].start()
    for send in sends:
        send.wait()


def pool_kernel(pool_rows, halo, maps, scale, keep_out, give_out):
    z, x, p = place()
    lane = lax.broadcasted_iota(jnp.int32, (1, LANES), 1)
    early = lane < GROUP_DIM
    current = pool_rows[...].astype(F32)
    two = jnp.concatenate([halo[...].astype(F32), current], axis=0)
    two = two + pltpu.roll(two, 1, 0)
    four = two + pltpu.roll(two, 2, 0)
    eight = four + pltpu.roll(four, 4, 0)
    sixteen = eight + pltpu.roll(eight, 8, 0)
    short = jnp.where(early, two, four)
    long = jnp.where(early, eight, sixteen)
    total = jnp.where(p == 0, short, long)[HALO:]
    window = jnp.where(early, 2, 4) * jnp.where(p == 0, 1, 4)
    row = lax.broadcasted_iota(jnp.int32, (BLOCK, 1), 0)
    divisor = jnp.minimum((z * BLOCK + row).astype(F32) + 1.0, window.astype(F32))
    means = (total / divisor - current).astype(BF16)
    empty = jnp.zeros((GROUP_DIM, GROUP_DIM), F32)
    upper = jnp.concatenate([maps[4 * x + 2 * p].astype(F32), empty], axis=1)
    lower = jnp.concatenate([empty, maps[4 * x + 2 * p + 1].astype(F32)], axis=1)
    weights = jnp.concatenate([upper, lower], axis=0).astype(BF16)
    pooled = (dot(means, weights) * scale[...]).reshape(CHIPS, 2, ROWS, LANES)
    even = pooled[:, 0].reshape(QROWS, LANES)
    odd = pooled[:, 1].reshape(QROWS, LANES)
    keep_out[...] = jnp.where(p == 0, even, odd)
    give_out[...] = jnp.where(p == 0, odd, even)


def join_kernel(parts, pool_own, pool_other, attended_out, squares_out):
    tail = jnp.zeros((HALO, QROWS), F32)
    for chip in range(CHIPS):
        tail = tail + parts[chip, QROWS:, :].astype(F32)
    columns = jnp.transpose(tail)
    squares = jnp.zeros((QROWS, LANES), F32)
    for slot in range(2):
        numer = jnp.zeros((QROWS, LANES), F32)
        for chip in range(CHIPS):
            numer = numer + parts[chip, :QROWS, slot * LANES : (slot + 1) * LANES].astype(F32)
        denom = columns[:, 2 * slot : 2 * slot + 1] + columns[:, 2 * slot + 1 : 2 * slot + 2]
        attended = numer / denom
        attended_out[slot] = attended
        squares = squares + attended * attended
    ones = jnp.ones((8, LANES), F32)
    exact = lax.Precision.HIGHEST
    line = lax.broadcasted_iota(jnp.int32, (8, QROWS), 0)
    mine = dot(ones, squares, ((1,), (1,)), exact)
    pooled = pool_own[...] * pool_own[...] + pool_other[...] * pool_other[...]
    pools = dot(ones, pooled, ((1,), (1,)), exact)
    for chip in range(CHIPS):
        squares_out[chip] = jnp.where(line < 4, mine, pools)


def mix_kernel(
    attended,
    pool_own,
    pool_other,
    squares,
    gain_a,
    gain_p,
    own_attention,
    own_pool,
    other_out,
    partial_out,
):
    _, _, p = place()
    total = jnp.transpose(squares[0] + squares[1] + squares[2] + squares[3])
    attention_factor = lax.rsqrt(total[:, 0:1] * (1.0 / (HEADS * VALUE_DIM)) + EPS)
    pool_factor = lax.rsqrt(total[:, 4:5] * (1.0 / (HEADS * VALUE_DIM)) + EPS)
    sides = []
    rows = other_out[2 * LANES :, :LANES].astype(F32)
    far = rows[0:4] + rows[4:8] + rows[8:12]
    for first, second, pooled, slot in (
        (gain_a[...], gain_p[...], pool_own, p),
        (far[0:1, :], far[1:2, :], pool_other, 1 - p),
    ):
        sides.append((attended[slot] * attention_factor * first).astype(BF16))
        sides.append((pooled[...] * pool_factor * second).astype(BF16))
    mine = jnp.concatenate(sides[:2], axis=1)
    theirs = jnp.concatenate(sides[2:], axis=1)
    step = 512
    for at in range(0, D, step):
        weights = jnp.concatenate(
            [own_attention[:, at : at + step], own_pool[:, at : at + step]], axis=0
        )
        both = dot(mine, weights) + dot(theirs, other_out[: 2 * LANES, at : at + step])
        partial_out[:, :, at : at + step] = both.astype(BF16).reshape(CHIPS, ROWS, step)


def sum_kernel(parts, out):
    total = parts[0].astype(F32) + parts[1].astype(F32)
    total = total + parts[2].astype(F32) + parts[3].astype(F32)
    out[0] = total.astype(BF16)


def local(
    tokens,
    input_gain,
    query_weight,
    latent_down,
    rotary_down,
    pool_down,
    key_up,
    value_up,
    query_gain,
    key_gain,
    pool_weight,
    pool_scale,
    attention_gain,
    pool_gain,
    attention_out,
    pool_out,
):
    inside, starts, turned, begins = (jnp.asarray(t) for t in angle_tables())

    def chip():
        return lax.axis_index("tp") // 2

    def up_to(step):
        return jnp.minimum(step, lax.axis_index("sp") // 4)

    normed, latent_rows, gain_row = whole(
        norm_kernel,
        (
            far((2 * CHIPS, ROWS, D), BF16),
            far((PACK, KV_LATENT), BF16),
            shape((8, LANES), F32),
        ),
        tokens,
        input_gain[None],
        latent_down,
        rotary_down.T,
        query_gain[None],
        room=56,
    )
    rows = among_all(normed)
    own_latents = lax.all_gather(latent_rows, "sp", axis=0, tiled=False)
    other_latents = to_partner(own_latents)

    queries, pool_rows, tail = whole(
        project_kernel,
        (
            far((2 * CHIPS, QROWS, LANES), BF16),
            far((BLOCK, LANES), BF16),
            far((HALO, LANES), BF16),
        ),
        rows,
        query_weight.T,
        pool_down,
        gain_row,
        inside,
        starts,
        specs=[AWAY] + [VECTOR] * 5,
        scratch=(
            pltpu.VMEM((2 * CHIPS, ROWS, D), BF16),
            pltpu.SemaphoreType.DMA((2,)),
        ),
        room=ROOM_PROJECT,
    )
    queries = among_all(queries)
    halo = lax.ppermute(tail, "sp", [(i, i + 1) for i in range(BLOCKS - 1)])

    latent_spec = pl.BlockSpec((4, PACK, KV_LATENT), lambda i: (up_to(i), 0, 0))
    expand = pl.pallas_call(
        expand_kernel,
        grid=(BLOCKS // 4,),
        out_shape=(far((HEADS, QK_DIM, KEYS), BF16), far((KEYS, KV_LATENT), BF16)),
        in_specs=[
            latent_spec,
            latent_spec,
            pl.BlockSpec((KV_LATENT, HEADS * NOPE_DIM), lambda i: (0, 0)),
            pl.BlockSpec((1, QK_DIM), lambda i: (0, 0)),
            pl.BlockSpec((2, 1, ROPE_DIM // 2, LANES), lambda i: (0, chip(), 0, 0)),
            pl.BlockSpec((2, 4, ROPE_DIM // 2, LANES), lambda i: (0, up_to(i), 0, 0)),
        ],
        out_specs=[
            pl.BlockSpec((HEADS, QK_DIM, QUAD), lambda i: (0, 0, up_to(i))),
            pl.BlockSpec((QUAD, KV_LATENT), lambda i: (up_to(i), 0)),
        ],
        scratch_shapes=[pltpu.VMEM((HEADS * NOPE_DIM, KV_LATENT), BF16)],
        compiler_params=pltpu.CompilerParams(vmem_limit_bytes=52 * MIB),
        name="expand",
    )
    keys, latents = expand(own_latents, other_latents, key_up, key_gain[None], turned, begins)

    numer = whole(
        attend_kernel,
        far((CHIPS, QROWS + HALO, 2 * LANES), BF16),
        queries,
        keys,
        latents,
        value_up,
        specs=[VECTOR, AWAY, AWAY, AWAY],
        outs=AWAY,
        scratch=(
            pltpu.VMEM((CHIPS, QROWS + HALO, 2 * LANES), BF16),
            pltpu.VMEM((HEADS, QK_DIM, KEYS), BF16),
            pltpu.VMEM((KEYS, KV_LATENT), BF16),
            pltpu.VMEM((KV_LATENT, HEADS * VALUE_DIM), BF16),
            pltpu.VMEM((HEADS, QROWS, KV_LATENT), F32),
            pltpu.VMEM((HEADS, QROWS, LANES), F32),
            pltpu.SemaphoreType.DMA((3, BLOCKS // 4 + 1)),
        ),
        room=58,
    )
    parts = among_chips(numer)

    pool_own, pool_give = whole(
        pool_kernel,
        (shape((QROWS, LANES), F32), shape((QROWS, LANES), F32)),
        pool_rows,
        halo,
        pool_weight,
        pool_scale[None],
    )
    pool_other = to_partner(pool_give)
    other_out = to_partner(
        whole(
            out_bundle_kernel,
            shape((2 * LANES + HALO, D), BF16),
            attention_out,
            pool_out,
            attention_gain[None],
            pool_gain[None],
        ),
    )
    attended, squares = whole(
        join_kernel,
        (shape((2, QROWS, LANES), F32), far((CHIPS, 8, QROWS), F32)),
        parts,
        pool_own,
        pool_other,
    )
    squares = among_chips(squares)
    partial = whole(
        mix_kernel,
        far((CHIPS, ROWS, D), BF16),
        attended,
        pool_own,
        pool_other,
        squares,
        attention_gain[None],
        pool_gain[None],
        attention_out,
        pool_out,
        other_out,
    )
    return whole(sum_kernel, shape((1, ROWS, D), BF16), among_chips(partial))


def solution(mesh):
    placed = (
        P("fs", ("sp", "tp"), None),
        P(),
        P(None, "tp"),
        P(),
        P(),
        P(None, "tp"),
        P(),
        P(),
        P(),
        P(),
        P(),
        P("tp"),
        P("tp"),
        P("tp"),
        P("tp", None),
        P("tp", None),
    )

    return jax.shard_map(
        local, mesh=mesh, in_specs=placed, out_specs=P("fs", ("sp", "tp"), None), check_vma=False
    )
```

```python
import math

import jax
import jax.numpy as jnp
import numpy as np
from jax import lax
from jax.experimental import pallas as pl
from jax.experimental.pallas import tpu as pltpu
from jax.sharding import PartitionSpec as P

HEADS = 8
NOPE_DIM = 64
ROPE_DIM = 32
VALUE_DIM = 128
KV_LATENT = 256
GROUP_DIM = 64
QK_DIM = 96
D = 2048
BLOCKS = 16
BLOCK = 512
CHIPS = 4
ROWS = 64
LANES = 128
QROWS = CHIPS * ROWS
KEYS = BLOCKS * 2 * ROWS
HALO = 16
PACK = ROWS + 8
QUAD = 4 * 2 * ROWS

EPS = 1e-06
THETA = 10000.0
SAME_CORE = [[0, 2, 4, 6], [1, 3, 5, 7]]
F32 = jnp.float32
BF16 = jnp.bfloat16


def angle_tables():
    half = ROPE_DIM // 2
    freq = np.zeros(LANES)
    inv = 1.0 / THETA ** (np.arange(half, dtype=np.float64) / half)
    freq[NOPE_DIM : NOPE_DIM + half] = inv
    freq[NOPE_DIM + half : QK_DIM] = inv
    inside = np.arange(BLOCK)[:, None] * freq[None, :]
    starts = (np.arange(BLOCKS) * BLOCK)[:, None] * freq[None, :]
    turned = (np.arange(BLOCK)[:, None] * inv[None, :]).reshape(CHIPS, 2 * ROWS, half)
    begins = (np.arange(BLOCKS) * BLOCK)[:, None] * inv[None, :]
    begins = np.broadcast_to(begins[:, :, None], (BLOCKS, half, LANES))
    tables = []
    for angle in (inside, starts, turned.transpose(0, 2, 1), begins):
        tables.append(np.stack([np.cos(angle), np.sin(angle)]).astype(np.float32))
    return tables


def among_chips(array):
    return lax.all_to_all(array, "tp", 0, 0, axis_index_groups=SAME_CORE, tiled=True)


def among_all(array):
    return lax.all_to_all(array, "tp", 0, 0, tiled=True)


def to_partner(array):
    return lax.ppermute(array, "tp", [(i, i ^ 1) for i in range(2 * CHIPS)])


MIB = 1024 * 1024
ROOM_PROJECT = 52
VECTOR = pl.BlockSpec(memory_space=pltpu.VMEM)
AWAY = pl.BlockSpec(memory_space=pltpu.HBM)


def whole(kernel, out_shape, *args, specs=None, outs=None, scratch=(), room=14):
    single = not isinstance(out_shape, (list, tuple))
    return pl.pallas_call(
        kernel,
        grid=() if specs is None else (1,),
        out_shape=out_shape,
        in_specs=[VECTOR] * len(args) if specs is None else specs,
        out_specs=outs or (VECTOR if single else [VECTOR] * len(out_shape)),
        scratch_shapes=list(scratch),
        compiler_params=pltpu.CompilerParams(vmem_limit_bytes=room * MIB),
    )(*args)


def place():
    member = lax.axis_index("tp")
    return lax.axis_index("sp"), member // 2, member % 2


def shape(dims, dtype):
    return jax.ShapeDtypeStruct(dims, dtype)


def far(dims, dtype):
    return pltpu.HBM(dims, dtype)


def dot(a, b, dims=((1,), (0,))):
    return lax.dot_general(a, b, (dims, ((), ())), preferred_element_type=F32)


def lane_totals(ones, values):
    high = values.astype(BF16)
    low = (values - high.astype(F32)).astype(BF16)
    return dot(ones, high, ((1,), (1,))) + dot(ones, low, ((1,), (1,)))


def turn(vectors, cosine, sine):
    lane = lax.broadcasted_iota(jnp.int32, vectors.shape, vectors.ndim - 1)
    half = ROPE_DIM // 2
    ahead = pltpu.roll(vectors, LANES - half, vectors.ndim - 1)
    behind = pltpu.roll(vectors, half, vectors.ndim - 1)
    return vectors * cosine + jnp.where(lane < NOPE_DIM + half, -ahead, behind) * sine


def at_block(inside_cos, inside_sin, start_cos, start_sin):
    cosine = start_cos * inside_cos - start_sin * inside_sin
    sine = start_sin * inside_cos + start_cos * inside_sin
    return cosine, sine


def norm_kernel(
    tokens, gain, latent_down, rotary_down, query_gain, normed_out, latent_out, gain_out
):
    source = tokens[0].astype(F32)
    scale = lax.rsqrt(jnp.mean(source * source, axis=-1, keepdims=True) + EPS)
    normed = (source * scale * gain[...]).astype(BF16)
    for member in range(2 * CHIPS):
        normed_out[member] = normed
    rotary = dot(rotary_down[...], normed, ((1,), (1,)))
    packed = jnp.concatenate([rotary[at : at + 8] for at in range(0, ROPE_DIM, 8)], axis=1)
    latent_out[ROWS:] = packed.astype(BF16)
    wide = jnp.concatenate([query_gain[...], jnp.zeros((1, LANES - QK_DIM), F32)], axis=1)
    wide = wide * (math.log2(math.e) / math.sqrt(QK_DIM))
    gain_out[...] = jnp.broadcast_to(wide, (8, LANES))
    latent_out[:ROWS] = dot(normed, latent_down[...]).astype(BF16)


def out_bundle_kernel(attention_out, pool_out, gain_a, gain_p, both):
    both[:LANES, :] = attention_out[...]
    both[LANES : 2 * LANES, :] = pool_out[...]
    rest = jnp.concatenate([gain_a[...], gain_p[...]] * 2, axis=0)
    rows = []
    for _ in range(3):
        piece = rest.astype(BF16)
        rest = rest - piece.astype(F32)
        rows.append(piece.astype(F32))
    rows.append(jnp.zeros((4, LANES), F32))
    rows = jnp.concatenate(rows, axis=0)
    both[2 * LANES :, :] = jnp.concatenate([rows] * (D // LANES), axis=1).astype(BF16)


def project_kernel(
    rows_far,
    query_down,
    pool_down,
    gain,
    inside,
    starts,
    query_out,
    pool_out,
    tail_out,
    rows,
    arrived,
):
    z, _, _ = place()
    per = CHIPS
    copies = []
    for part in range(2):
        span = pl.ds(part * per, per)
        copies.append(
            pltpu.make_async_copy(rows_far.at[span], rows.at[span], arrived.at[part])
        )
        copies[-1].start()
    start_cos = starts[0, pl.ds(z, 1), :]
    start_sin = starts[1, pl.ds(z, 1), :]
    cosine, sine = at_block(inside[0], inside[1], start_cos, start_sin)
    empty = jnp.zeros((LANES - QK_DIM, D), BF16)
    query_wide = jnp.concatenate([query_down[...], empty], axis=0)
    half = per * ROWS
    for part in range(2):
        copies[part].wait()
        piece = rows[part * per : (part + 1) * per].reshape(half, D)
        raw = dot(piece, query_wide, ((1,), (1,)))
        square = jnp.sum(raw * raw, axis=-1, keepdims=True) * (1.0 / QK_DIM)
        normal = raw * lax.rsqrt(square + EPS) * gain[0:1, :]
        span = slice(part * half, (part + 1) * half)
        queries = turn(normal, cosine[span], sine[span]).astype(BF16)
        for member in range(per):
            mine = queries[member * ROWS : (member + 1) * ROWS]
            side, chip = member % 2, (part * per + member) // 2
            for target in range(CHIPS):
                query_out[2 * target + side, chip * ROWS : (chip + 1) * ROWS] = mine
        result = dot(piece, pool_down[...]).astype(BF16)
        pool_out[part * half : (part + 1) * half] = result
    tail_out[...] = result[half - HALO :]


def expand_kernel(own, other, key_up, gain, inside, starts, keys_out, latent_out, key_up_t):
    z, _, p = place()
    step = pl.program_id(0)

    @pl.when(step == 0)
    def _():
        key_up_t[...] = jnp.transpose(key_up[...].astype(F32)).astype(BF16)

    @pl.when(step <= z // 4)
    def _():
        wide_gain = jnp.concatenate([gain[...], jnp.zeros((1, LANES - QK_DIM), F32)], axis=1)
        wide_gain = jnp.broadcast_to(wide_gain * math.sqrt(QK_DIM), (8, LANES))
        column = jnp.transpose(wide_gain)[:, 0:1]
        half = ROPE_DIM // 2
        latents, rotaries, cosines, sines = [], [], [], []
        for k in range(4):
            mine, theirs = own[k].astype(F32), other[k].astype(F32)
            for side in (jnp.where(p == 0, mine, theirs), jnp.where(p == 0, theirs, mine)):
                latents.append(side[:ROWS])
                rotaries.append(
                    jnp.concatenate(
                        [side[ROWS:, at : at + ROWS] for at in range(0, KV_LATENT, ROWS)], axis=0
                    )
                )
            cosine, sine = at_block(inside[0, 0], inside[1, 0], starts[0, k], starts[1, k])
            cosines.append(cosine)
            sines.append(sine)
        latent = jnp.concatenate(latents, axis=0)
        rotary = jnp.concatenate(rotaries, axis=1)
        cosine = jnp.concatenate(cosines, axis=1)
        sine = jnp.concatenate(sines, axis=1)
        scale = lax.rsqrt(jnp.mean(latent * latent, axis=-1, keepdims=True) + EPS)
        normed = (latent * scale).astype(BF16)
        latent_out[...] = normed
        shared = jnp.sum(rotary * rotary, axis=0, keepdims=True) + QK_DIM * EPS
        ahead = rotary[:half] * column[NOPE_DIM : NOPE_DIM + half]
        behind = rotary[half:] * column[NOPE_DIM + half : QK_DIM]
        turned = jnp.concatenate(
            [ahead * cosine - behind * sine, behind * cosine + ahead * sine], axis=0
        )
        plain_gain = jnp.broadcast_to(column[:NOPE_DIM], (NOPE_DIM, QUAD))
        for head in range(HEADS):
            rows = key_up_t[head * NOPE_DIM : (head + 1) * NOPE_DIM, :]
            part = dot(rows, normed, ((1,), (1,)))
            factor = lax.rsqrt(jnp.sum(part * part, axis=0, keepdims=True) + shared)
            keys_out[head, :NOPE_DIM, :] = (part * plain_gain * factor).astype(BF16)
            keys_out[head, NOPE_DIM:, :] = (turned * factor).astype(BF16)


def attend_kernel(
    queries,
    keys_far,
    latents_far,
    value_far,
    out_far,
    out,
    keys,
    latents,
    value_up,
    sums,
    totals,
    arrived,
):
    z, x, p = place()
    wide = QUAD
    pair = z // 4

    def copies(index):
        at = pl.multiple_of(index * wide, wide)
        return (
            pltpu.make_async_copy(
                keys_far.at[:, :, pl.ds(at, wide)],
                keys.at[:, :, pl.ds(at, wide)],
                arrived.at[0, index],
            ),
            pltpu.make_async_copy(
                latents_far.at[pl.ds(at, wide), :],
                latents.at[pl.ds(at, wide), :],
                arrived.at[1, index],
            ),
        )

    def fetch(index, carry):
        for copy in copies(pair - index):
            copy.start()
        return carry

    lax.fori_loop(0, pair + 1, fetch, 0)
    value_copy = pltpu.make_async_copy(value_far, value_up, arrived.at[0, BLOCKS // 4])
    value_copy.start()

    def chunk(index, mask, first, width=QUAD):
        at = pl.multiple_of(index * wide, wide)
        for copy in copies(index):
            copy.wait()
        latent = latents[pl.ds(at, width), :]
        for head in range(HEADS):
            scores = dot(queries[head, :, :QK_DIM], keys[head, :, pl.ds(at, width)])
            weights = jnp.exp2(scores)
            if mask is not None:
                weights = jnp.where(mask, weights, 0.0)
            part = weights[:, :LANES]
            for lanes in range(LANES, width, LANES):
                part = part + weights[:, lanes : lanes + LANES]
            numer = dot(weights.astype(BF16), latent)
            if first:
                totals[head] = part
                sums[head] = numer
            else:
                totals[head] += part
                sums[head] += numer

    def last(width):
        row = lax.broadcasted_iota(jnp.int32, (QROWS, width), 0)
        col = lax.broadcasted_iota(jnp.int32, (QROWS, width), 1)
        query_pos = z * BLOCK + (row // ROWS) * (2 * ROWS) + p * ROWS + row % ROWS
        key_pos = (4 * pair + col // (2 * ROWS)) * BLOCK + x * (2 * ROWS) + col % (2 * ROWS)
        chunk(pair, key_pos <= query_pos, True, width)

    @pl.when(z % 4 < 2)
    def _():
        last(QUAD // 2)

    @pl.when(z % 4 >= 2)
    def _():
        last(QUAD)

    def body(index, carry):
        chunk(pair - 1 - index, None, False)
        return carry

    lax.fori_loop(0, pair, body, 0)
    value_copy.wait()
    sends = []
    ones = jnp.ones((HALO, LANES), BF16)
    line = lax.broadcasted_iota(jnp.int32, (HALO, QROWS), 0)
    for chip in range(CHIPS):
        tail = jnp.zeros((HALO, QROWS), F32)
        for slot in range(2):
            head = 2 * chip + slot
            values = value_up[:, head * VALUE_DIM : (head + 1) * VALUE_DIM]
            numer = dot(sums[head].astype(BF16), values)
            out[chip, :QROWS, slot * LANES : (slot + 1) * LANES] = numer.astype(BF16)
            denom = lane_totals(ones, totals[head])
            high = denom.astype(BF16).astype(F32)
            tail = jnp.where(line == 2 * slot, high, tail)
            tail = jnp.where(line == 2 * slot + 1, denom - high, tail)
        out[chip, QROWS:, :] = tail.astype(BF16)
        sends.append(pltpu.make_async_copy(out.at[chip], out_far.at[chip], arrived.at[2, chip]))
        sends[-1].start()
    for send in sends:
        send.wait()


def pool_kernel(pool_rows, halo, maps, scale, keep_out, give_out):
    z, x, p = place()
    lane = lax.broadcasted_iota(jnp.int32, (1, LANES), 1)
    early = lane < GROUP_DIM
    current = pool_rows[...].astype(F32)
    two = jnp.concatenate([halo[...].astype(F32), current], axis=0)
    two = two + pltpu.roll(two, 1, 0)
    four = two + pltpu.roll(two, 2, 0)
    eight = four + pltpu.roll(four, 4, 0)
    sixteen = eight + pltpu.roll(eight, 8, 0)
    short = jnp.where(early, two, four)
    long = jnp.where(early, eight, sixteen)
    total = jnp.where(p == 0, short, long)[HALO:]
    window = jnp.where(early, 2, 4) * jnp.where(p == 0, 1, 4)
    row = lax.broadcasted_iota(jnp.int32, (BLOCK, 1), 0)
    divisor = jnp.minimum((z * BLOCK + row).astype(F32) + 1.0, window.astype(F32))
    means = (total / divisor - current).astype(BF16)
    empty = jnp.zeros((GROUP_DIM, GROUP_DIM), F32)
    upper = jnp.concatenate([maps[4 * x + 2 * p].astype(F32), empty], axis=1)
    lower = jnp.concatenate([empty, maps[4 * x + 2 * p + 1].astype(F32)], axis=1)
    weights = jnp.concatenate([upper, lower], axis=0).astype(BF16)
    pooled = (dot(means, weights) * scale[...]).reshape(CHIPS, 2, ROWS, LANES)
    even = pooled[:, 0].reshape(QROWS, LANES)
    odd = pooled[:, 1].reshape(QROWS, LANES)
    keep_out[...] = jnp.where(p == 0, even, odd)
    give_out[...] = jnp.where(p == 0, odd, even)


def join_kernel(parts, pool_own, pool_other, attended_out, squares_out):
    tail = jnp.zeros((HALO, QROWS), F32)
    for chip in range(CHIPS):
        tail = tail + parts[chip, QROWS:, :].astype(F32)
    columns = jnp.transpose(tail)
    squares = jnp.zeros((QROWS, LANES), F32)
    for slot in range(2):
        numer = jnp.zeros((QROWS, LANES), F32)
        for chip in range(CHIPS):
            numer = numer + parts[chip, :QROWS, slot * LANES : (slot + 1) * LANES].astype(F32)
        denom = columns[:, 2 * slot : 2 * slot + 1] + columns[:, 2 * slot + 1 : 2 * slot + 2]
        attended = numer / denom
        attended_out[slot] = attended
        squares = squares + attended * attended
    ones = jnp.ones((HALO, LANES), BF16)
    line = lax.broadcasted_iota(jnp.int32, (8, QROWS), 0)
    mine = lane_totals(ones, squares)[:8]
    pooled = pool_own[...] * pool_own[...] + pool_other[...] * pool_other[...]
    pools = lane_totals(ones, pooled)[:8]
    for chip in range(CHIPS):
        squares_out[chip] = jnp.where(line < 4, mine, pools)


def mix_kernel(
    attended,
    pool_own,
    pool_other,
    squares,
    gain_a,
    gain_p,
    own_attention,
    own_pool,
    other_out,
    partial_out,
):
    _, _, p = place()
    total = jnp.transpose(squares[0] + squares[1] + squares[2] + squares[3])
    attention_factor = lax.rsqrt(total[:, 0:1] * (1.0 / (HEADS * VALUE_DIM)) + EPS)
    pool_factor = lax.rsqrt(total[:, 4:5] * (1.0 / (HEADS * VALUE_DIM)) + EPS)
    sides = []
    rows = other_out[2 * LANES :, :LANES].astype(F32)
    far = rows[0:4] + rows[4:8] + rows[8:12]
    for first, second, pooled, slot in (
        (gain_a[...], gain_p[...], pool_own, p),
        (far[0:1, :], far[1:2, :], pool_other, 1 - p),
    ):
        sides.append((attended[slot] * attention_factor * first).astype(BF16))
        sides.append((pooled[...] * pool_factor * second).astype(BF16))
    mine = jnp.concatenate(sides[:2], axis=1)
    theirs = jnp.concatenate(sides[2:], axis=1)
    step = 512
    for at in range(0, D, step):
        weights = jnp.concatenate(
            [own_attention[:, at : at + step], own_pool[:, at : at + step]], axis=0
        )
        both = dot(mine, weights) + dot(theirs, other_out[: 2 * LANES, at : at + step])
        partial_out[:, :, at : at + step] = both.astype(BF16).reshape(CHIPS, ROWS, step)


def sum_kernel(parts, out):
    total = parts[0].astype(F32) + parts[1].astype(F32)
    total = total + parts[2].astype(F32) + parts[3].astype(F32)
    out[0] = total.astype(BF16)


def local(
    tokens,
    input_gain,
    query_weight,
    latent_down,
    rotary_down,
    pool_down,
    key_up,
    value_up,
    query_gain,
    key_gain,
    pool_weight,
    pool_scale,
    attention_gain,
    pool_gain,
    attention_out,
    pool_out,
):
    inside, starts, turned, begins = (jnp.asarray(t) for t in angle_tables())

    def chip():
        return lax.axis_index("tp") // 2

    def up_to(step):
        return jnp.minimum(step, lax.axis_index("sp") // 4)

    normed, latent_rows, gain_row = whole(
        norm_kernel,
        (
            far((2 * CHIPS, ROWS, D), BF16),
            far((PACK, KV_LATENT), BF16),
            shape((8, LANES), F32),
        ),
        tokens,
        input_gain[None],
        latent_down,
        rotary_down.T,
        query_gain[None],
        room=56,
    )
    rows = among_all(normed)
    own_latents = lax.all_gather(latent_rows, "sp", axis=0, tiled=False)
    other_latents = to_partner(own_latents)

    queries, pool_rows, tail = whole(
        project_kernel,
        (
            far((2 * CHIPS, QROWS, LANES), BF16),
            far((BLOCK, LANES), BF16),
            far((HALO, LANES), BF16),
        ),
        rows,
        query_weight.T,
        pool_down,
        gain_row,
        inside,
        starts,
        specs=[AWAY] + [VECTOR] * 5,
        scratch=(
            pltpu.VMEM((2 * CHIPS, ROWS, D), BF16),
            pltpu.SemaphoreType.DMA((2,)),
        ),
        room=ROOM_PROJECT,
    )
    queries = among_all(queries)
    halo = lax.ppermute(tail, "sp", [(i, i + 1) for i in range(BLOCKS - 1)])

    latent_spec = pl.BlockSpec((4, PACK, KV_LATENT), lambda i: (up_to(i), 0, 0))
    expand = pl.pallas_call(
        expand_kernel,
        grid=(BLOCKS // 4,),
        out_shape=(far((HEADS, QK_DIM, KEYS), BF16), far((KEYS, KV_LATENT), BF16)),
        in_specs=[
            latent_spec,
            latent_spec,
            pl.BlockSpec((KV_LATENT, HEADS * NOPE_DIM), lambda i: (0, 0)),
            pl.BlockSpec((1, QK_DIM), lambda i: (0, 0)),
            pl.BlockSpec((2, 1, ROPE_DIM // 2, LANES), lambda i: (0, chip(), 0, 0)),
            pl.BlockSpec((2, 4, ROPE_DIM // 2, LANES), lambda i: (0, up_to(i), 0, 0)),
        ],
        out_specs=[
            pl.BlockSpec((HEADS, QK_DIM, QUAD), lambda i: (0, 0, up_to(i))),
            pl.BlockSpec((QUAD, KV_LATENT), lambda i: (up_to(i), 0)),
        ],
        scratch_shapes=[pltpu.VMEM((HEADS * NOPE_DIM, KV_LATENT), BF16)],
        compiler_params=pltpu.CompilerParams(vmem_limit_bytes=52 * MIB),
        name="expand",
    )
    keys, latents = expand(own_latents, other_latents, key_up, key_gain[None], turned, begins)

    numer = whole(
        attend_kernel,
        far((CHIPS, QROWS + HALO, 2 * LANES), BF16),
        queries,
        keys,
        latents,
        value_up,
        specs=[VECTOR, AWAY, AWAY, AWAY],
        outs=AWAY,
        scratch=(
            pltpu.VMEM((CHIPS, QROWS + HALO, 2 * LANES), BF16),
            pltpu.VMEM((HEADS, QK_DIM, KEYS), BF16),
            pltpu.VMEM((KEYS, KV_LATENT), BF16),
            pltpu.VMEM((KV_LATENT, HEADS * VALUE_DIM), BF16),
            pltpu.VMEM((HEADS, QROWS, KV_LATENT), F32),
            pltpu.VMEM((HEADS, QROWS, LANES), F32),
            pltpu.SemaphoreType.DMA((3, BLOCKS // 4 + 1)),
        ),
        room=53,
    )
    parts = among_chips(numer)

    pool_own, pool_give = whole(
        pool_kernel,
        (shape((QROWS, LANES), F32), shape((QROWS, LANES), F32)),
        pool_rows,
        halo,
        pool_weight,
        pool_scale[None],
    )
    pool_other = to_partner(pool_give)
    other_out = to_partner(
        whole(
            out_bundle_kernel,
            shape((2 * LANES + HALO, D), BF16),
            attention_out,
            pool_out,
            attention_gain[None],
            pool_gain[None],
        ),
    )
    attended, squares = whole(
        join_kernel,
        (shape((2, QROWS, LANES), F32), far((CHIPS, 8, QROWS), F32)),
        parts,
        pool_own,
        pool_other,
    )
    squares = among_chips(squares)
    partial = whole(
        mix_kernel,
        far((CHIPS, ROWS, D), BF16),
        attended,
        pool_own,
        pool_other,
        squares,
        attention_gain[None],
        pool_gain[None],
        attention_out,
        pool_out,
        other_out,
    )
    return whole(sum_kernel, shape((1, ROWS, D), BF16), among_chips(partial))


def solution(mesh):
    placed = (
        P("fs", ("sp", "tp"), None),
        P(),
        P(None, "tp"),
        P(),
        P(),
        P(None, "tp"),
        P(),
        P(),
        P(),
        P(),
        P(),
        P("tp"),
        P("tp"),
        P("tp"),
        P("tp", None),
        P("tp", None),
    )

    return jax.shard_map(
        local, mesh=mesh, in_specs=placed, out_specs=P("fs", ("sp", "tp"), None), check_vma=False
    )
```

```python
import math

import jax
import jax.numpy as jnp
import numpy as np
from jax import lax
from jax.experimental import pallas as pl
from jax.experimental.pallas import tpu as pltpu
from jax.sharding import PartitionSpec as P

HEADS = 8
NOPE_DIM = 64
ROPE_DIM = 32
VALUE_DIM = 128
KV_LATENT = 256
GROUP_DIM = 64
QK_DIM = 96
D = 2048
BLOCKS = 16
BLOCK = 512
CHIPS = 4
ROWS = 64
LANES = 128
QROWS = CHIPS * ROWS
KEYS = BLOCKS * 2 * ROWS
HALO = 16
PACK = ROWS + 8
QUAD = 4 * 2 * ROWS

EPS = 1e-06
THETA = 10000.0
SAME_CORE = [[0, 2, 4, 6], [1, 3, 5, 7]]
F32 = jnp.float32
BF16 = jnp.bfloat16


def angle_tables():
    half = ROPE_DIM // 2
    freq = np.zeros(LANES)
    inv = 1.0 / THETA ** (np.arange(half, dtype=np.float64) / half)
    freq[NOPE_DIM : NOPE_DIM + half] = inv
    freq[NOPE_DIM + half : QK_DIM] = inv
    inside = np.arange(BLOCK)[:, None] * freq[None, :]
    starts = (np.arange(BLOCKS) * BLOCK)[:, None] * freq[None, :]
    turned = (np.arange(BLOCK)[:, None] * inv[None, :]).reshape(CHIPS, 2 * ROWS, half)
    begins = (np.arange(BLOCKS) * BLOCK)[:, None] * inv[None, :]
    begins = np.broadcast_to(begins[:, :, None], (BLOCKS, half, LANES))
    tables = []
    for angle in (inside, starts, turned.transpose(0, 2, 1), begins):
        tables.append(np.stack([np.cos(angle), np.sin(angle)]).astype(np.float32))
    return tables


def among_chips(array):
    return lax.all_to_all(array, "tp", 0, 0, axis_index_groups=SAME_CORE, tiled=True)


def among_all(array):
    return lax.all_to_all(array, "tp", 0, 0, tiled=True)


def to_partner(array):
    return lax.ppermute(array, "tp", [(i, i ^ 1) for i in range(2 * CHIPS)])


MIB = 1024 * 1024
ROOM_PROJECT = 52
VECTOR = pl.BlockSpec(memory_space=pltpu.VMEM)
AWAY = pl.BlockSpec(memory_space=pltpu.HBM)


def whole(kernel, out_shape, *args, specs=None, outs=None, scratch=(), room=14):
    single = not isinstance(out_shape, (list, tuple))
    return pl.pallas_call(
        kernel,
        grid=() if specs is None else (1,),
        out_shape=out_shape,
        in_specs=[VECTOR] * len(args) if specs is None else specs,
        out_specs=outs or (VECTOR if single else [VECTOR] * len(out_shape)),
        scratch_shapes=list(scratch),
        compiler_params=pltpu.CompilerParams(vmem_limit_bytes=room * MIB),
    )(*args)


def place():
    member = lax.axis_index("tp")
    return lax.axis_index("sp"), member // 2, member % 2


def shape(dims, dtype):
    return jax.ShapeDtypeStruct(dims, dtype)


def far(dims, dtype):
    return pltpu.HBM(dims, dtype)


def dot(a, b, dims=((1,), (0,))):
    return lax.dot_general(a, b, (dims, ((), ())), preferred_element_type=F32)


def lane_totals(ones, values):
    high = values.astype(BF16)
    low = (values - high.astype(F32)).astype(BF16)
    return dot(ones, high, ((1,), (1,))) + dot(ones, low, ((1,), (1,)))


def turn(vectors, cosine, sine):
    lane = lax.broadcasted_iota(jnp.int32, vectors.shape, vectors.ndim - 1)
    half = ROPE_DIM // 2
    ahead = pltpu.roll(vectors, LANES - half, vectors.ndim - 1)
    behind = pltpu.roll(vectors, half, vectors.ndim - 1)
    return vectors * cosine + jnp.where(lane < NOPE_DIM + half, -ahead, behind) * sine


def at_block(inside_cos, inside_sin, start_cos, start_sin):
    cosine = start_cos * inside_cos - start_sin * inside_sin
    sine = start_sin * inside_cos + start_cos * inside_sin
    return cosine, sine


def norm_kernel(
    tokens, gain, latent_down, rotary_down, query_gain, normed_out, latent_out, gain_out
):
    source = tokens[0].astype(F32)
    scale = lax.rsqrt(jnp.mean(source * source, axis=-1, keepdims=True) + EPS)
    normed = (source * scale * gain[...]).astype(BF16)
    for member in range(2 * CHIPS):
        normed_out[member] = normed
    rotary = dot(rotary_down[...], normed, ((1,), (1,)))
    packed = jnp.concatenate([rotary[at : at + 8] for at in range(0, ROPE_DIM, 8)], axis=1)
    latent_out[ROWS:] = packed.astype(BF16)
    wide = jnp.concatenate([query_gain[...], jnp.zeros((1, LANES - QK_DIM), F32)], axis=1)
    wide = wide * (math.log2(math.e) / math.sqrt(QK_DIM))
    gain_out[...] = jnp.broadcast_to(wide, (8, LANES))
    latent_out[:ROWS] = dot(normed, latent_down[...]).astype(BF16)


def out_bundle_kernel(attention_out, pool_out, gain_a, gain_p, both):
    both[:LANES, :] = attention_out[...]
    both[LANES : 2 * LANES, :] = pool_out[...]
    rest = jnp.concatenate([gain_a[...], gain_p[...]] * 2, axis=0)
    rows = []
    for _ in range(3):
        piece = rest.astype(BF16)
        rest = rest - piece.astype(F32)
        rows.append(piece.astype(F32))
    rows.append(jnp.zeros((4, LANES), F32))
    rows = jnp.concatenate(rows, axis=0)
    both[2 * LANES :, :] = jnp.concatenate([rows] * (D // LANES), axis=1).astype(BF16)


def project_kernel(
    rows_far,
    query_down,
    pool_down,
    gain,
    inside,
    starts,
    query_out,
    pool_out,
    tail_out,
    rows,
    arrived,
):
    z, _, _ = place()
    per = CHIPS
    copies = []
    for part in range(2):
        span = pl.ds(part * per, per)
        copies.append(
            pltpu.make_async_copy(rows_far.at[span], rows.at[span], arrived.at[part])
        )
        copies[-1].start()
    start_cos = starts[0, pl.ds(z, 1), :]
    start_sin = starts[1, pl.ds(z, 1), :]
    cosine, sine = at_block(inside[0], inside[1], start_cos, start_sin)
    empty = jnp.zeros((LANES - QK_DIM, D), BF16)
    query_wide = jnp.concatenate([query_down[...], empty], axis=0)
    half = per * ROWS
    for part in range(2):
        copies[part].wait()
        piece = rows[part * per : (part + 1) * per].reshape(half, D)
        raw = dot(piece, query_wide, ((1,), (1,)))
        square = jnp.sum(raw * raw, axis=-1, keepdims=True) * (1.0 / QK_DIM)
        normal = raw * lax.rsqrt(square + EPS) * gain[0:1, :]
        span = slice(part * half, (part + 1) * half)
        queries = turn(normal, cosine[span], sine[span]).astype(BF16)
        for member in range(per):
            mine = queries[member * ROWS : (member + 1) * ROWS]
            side, chip = member % 2, (part * per + member) // 2
            for target in range(CHIPS):
                query_out[2 * target + side, chip * ROWS : (chip + 1) * ROWS] = mine
        result = dot(piece, pool_down[...]).astype(BF16)
        pool_out[part * half : (part + 1) * half] = result
    tail_out[...] = result[half - HALO :]


def expand_kernel(own, other, key_up, gain, inside, starts, keys_out, latent_out, key_up_t):
    z, _, p = place()
    step = pl.program_id(0)

    @pl.when(step == 0)
    def _():
        key_up_t[...] = jnp.transpose(key_up[...].astype(F32)).astype(BF16)

    @pl.when(step <= z // 4)
    def _():
        wide_gain = jnp.concatenate([gain[...], jnp.zeros((1, LANES - QK_DIM), F32)], axis=1)
        wide_gain = jnp.broadcast_to(wide_gain * math.sqrt(QK_DIM), (8, LANES))
        column = jnp.transpose(wide_gain)[:, 0:1]
        half = ROPE_DIM // 2
        latents, rotaries, cosines, sines = [], [], [], []
        for k in range(4):
            mine, theirs = own[k].astype(F32), other[k].astype(F32)
            for side in (jnp.where(p == 0, mine, theirs), jnp.where(p == 0, theirs, mine)):
                latents.append(side[:ROWS])
                rotaries.append(
                    jnp.concatenate(
                        [side[ROWS:, at : at + ROWS] for at in range(0, KV_LATENT, ROWS)], axis=0
                    )
                )
            cosine, sine = at_block(inside[0, 0], inside[1, 0], starts[0, k], starts[1, k])
            cosines.append(cosine)
            sines.append(sine)
        latent = jnp.concatenate(latents, axis=0)
        rotary = jnp.concatenate(rotaries, axis=1)
        cosine = jnp.concatenate(cosines, axis=1)
        sine = jnp.concatenate(sines, axis=1)
        scale = lax.rsqrt(jnp.mean(latent * latent, axis=-1, keepdims=True) + EPS)
        normed = (latent * scale).astype(BF16)
        latent_out[...] = normed
        shared = jnp.sum(rotary * rotary, axis=0, keepdims=True) + QK_DIM * EPS
        ahead = rotary[:half] * column[NOPE_DIM : NOPE_DIM + half]
        behind = rotary[half:] * column[NOPE_DIM + half : QK_DIM]
        turned = jnp.concatenate(
            [ahead * cosine - behind * sine, behind * cosine + ahead * sine], axis=0
        )
        plain_gain = jnp.broadcast_to(column[:NOPE_DIM], (NOPE_DIM, QUAD))
        for head in range(HEADS):
            rows = key_up_t[head * NOPE_DIM : (head + 1) * NOPE_DIM, :]
            part = dot(rows, normed, ((1,), (1,)))
            factor = lax.rsqrt(jnp.sum(part * part, axis=0, keepdims=True) + shared)
            keys_out[head, :NOPE_DIM, :] = (part * plain_gain * factor).astype(BF16)
            keys_out[head, NOPE_DIM:, :] = (turned * factor).astype(BF16)


def attend_kernel(
    queries,
    keys_far,
    latents_far,
    value_far,
    out_far,
    out,
    keys,
    latents,
    value_up,
    sums,
    totals,
    arrived,
):
    z, x, p = place()
    wide = QUAD
    pair = z // 4

    def copies(index):
        at = pl.multiple_of(index * wide, wide)
        return (
            pltpu.make_async_copy(
                keys_far.at[:, :, pl.ds(at, wide)],
                keys.at[:, :, pl.ds(at, wide)],
                arrived.at[0, index],
            ),
            pltpu.make_async_copy(
                latents_far.at[pl.ds(at, wide), :],
                latents.at[pl.ds(at, wide), :],
                arrived.at[1, index],
            ),
        )

    def fetch(index, carry):
        for copy in copies(pair - index):
            copy.start()
        return carry

    lax.fori_loop(0, pair + 1, fetch, 0)
    value_copy = pltpu.make_async_copy(value_far, value_up, arrived.at[0, BLOCKS // 4])
    value_copy.start()

    def chunk(index, mask, first, width=QUAD):
        at = pl.multiple_of(index * wide, wide)
        for copy in copies(index):
            copy.wait()
        latent = latents[pl.ds(at, width), :]
        for head in range(HEADS):
            scores = dot(queries[head, :, :QK_DIM], keys[head, :, pl.ds(at, width)])
            weights = jnp.exp2(scores)
            if mask is not None:
                weights = jnp.where(mask, weights, 0.0)
            part = weights[:, :LANES]
            for lanes in range(LANES, width, LANES):
                part = part + weights[:, lanes : lanes + LANES]
            numer = dot(weights.astype(BF16), latent)
            if first:
                totals[head] = part
                sums[head] = numer
            else:
                totals[head] += part
                sums[head] += numer

    def last(width):
        row = lax.broadcasted_iota(jnp.int32, (QROWS, width), 0)
        col = lax.broadcasted_iota(jnp.int32, (QROWS, width), 1)
        query_pos = z * BLOCK + (row // ROWS) * (2 * ROWS) + p * ROWS + row % ROWS
        key_pos = (4 * pair + col // (2 * ROWS)) * BLOCK + x * (2 * ROWS) + col % (2 * ROWS)
        chunk(pair, key_pos <= query_pos, True, width)

    @pl.when(z % 4 == 0)
    def _():
        last(QUAD // 4)

    @pl.when(z % 4 == 1)
    def _():
        last(QUAD // 2)

    @pl.when(z % 4 >= 2)
    def _():
        last(QUAD)

    def body(index, carry):
        chunk(pair - 1 - index, None, False)
        return carry

    lax.fori_loop(0, pair, body, 0)
    value_copy.wait()
    sends = []
    ones = jnp.ones((HALO, LANES), BF16)
    line = lax.broadcasted_iota(jnp.int32, (HALO, QROWS), 0)
    for chip in range(CHIPS):
        tail = jnp.zeros((HALO, QROWS), F32)
        for slot in range(2):
            head = 2 * chip + slot
            values = value_up[:, head * VALUE_DIM : (head + 1) * VALUE_DIM]
            numer = dot(sums[head].astype(BF16), values)
            out[chip, :QROWS, slot * LANES : (slot + 1) * LANES] = numer.astype(BF16)
            denom = lane_totals(ones, totals[head])
            high = denom.astype(BF16).astype(F32)
            tail = jnp.where(line == 2 * slot, high, tail)
            tail = jnp.where(line == 2 * slot + 1, denom - high, tail)
        out[chip, QROWS:, :] = tail.astype(BF16)
        sends.append(pltpu.make_async_copy(out.at[chip], out_far.at[chip], arrived.at[2, chip]))
        sends[-1].start()
    for send in sends:
        send.wait()


def pool_kernel(pool_rows, halo, maps, scale, keep_out, give_out):
    z, x, p = place()
    lane = lax.broadcasted_iota(jnp.int32, (1, LANES), 1)
    early = lane < GROUP_DIM
    current = pool_rows[...].astype(F32)
    two = jnp.concatenate([halo[...].astype(F32), current], axis=0)
    two = two + pltpu.roll(two, 1, 0)
    four = two + pltpu.roll(two, 2, 0)
    eight = four + pltpu.roll(four, 4, 0)
    sixteen = eight + pltpu.roll(eight, 8, 0)
    short = jnp.where(early, two, four)
    long = jnp.where(early, eight, sixteen)
    total = jnp.where(p == 0, short, long)[HALO:]
    window = jnp.where(early, 2, 4) * jnp.where(p == 0, 1, 4)
    row = lax.broadcasted_iota(jnp.int32, (BLOCK, 1), 0)
    divisor = jnp.minimum((z * BLOCK + row).astype(F32) + 1.0, window.astype(F32))
    means = (total / divisor - current).astype(BF16)
    empty = jnp.zeros((GROUP_DIM, GROUP_DIM), F32)
    upper = jnp.concatenate([maps[4 * x + 2 * p].astype(F32), empty], axis=1)
    lower = jnp.concatenate([empty, maps[4 * x + 2 * p + 1].astype(F32)], axis=1)
    weights = jnp.concatenate([upper, lower], axis=0).astype(BF16)
    pooled = (dot(means, weights) * scale[...]).reshape(CHIPS, 2, ROWS, LANES)
    even = pooled[:, 0].reshape(QROWS, LANES)
    odd = pooled[:, 1].reshape(QROWS, LANES)
    keep_out[...] = jnp.where(p == 0, even, odd)
    give_out[...] = jnp.where(p == 0, odd, even)


def join_kernel(parts, pool_own, pool_other, attended_out, squares_out):
    tail = jnp.zeros((HALO, QROWS), F32)
    for chip in range(CHIPS):
        tail = tail + parts[chip, QROWS:, :].astype(F32)
    columns = jnp.transpose(tail)
    squares = jnp.zeros((QROWS, LANES), F32)
    for slot in range(2):
        numer = jnp.zeros((QROWS, LANES), F32)
        for chip in range(CHIPS):
            numer = numer + parts[chip, :QROWS, slot * LANES : (slot + 1) * LANES].astype(F32)
        denom = columns[:, 2 * slot : 2 * slot + 1] + columns[:, 2 * slot + 1 : 2 * slot + 2]
        attended = numer / denom
        attended_out[slot] = attended
        squares = squares + attended * attended
    ones = jnp.ones((HALO, LANES), BF16)
    line = lax.broadcasted_iota(jnp.int32, (8, QROWS), 0)
    mine = lane_totals(ones, squares)[:8]
    pooled = pool_own[...] * pool_own[...] + pool_other[...] * pool_other[...]
    pools = lane_totals(ones, pooled)[:8]
    for chip in range(CHIPS):
        squares_out[chip] = jnp.where(line < 4, mine, pools)


def mix_kernel(
    attended,
    pool_own,
    pool_other,
    squares,
    gain_a,
    gain_p,
    own_attention,
    own_pool,
    other_out,
    partial_out,
):
    _, _, p = place()
    total = jnp.transpose(squares[0] + squares[1] + squares[2] + squares[3])
    attention_factor = lax.rsqrt(total[:, 0:1] * (1.0 / (HEADS * VALUE_DIM)) + EPS)
    pool_factor = lax.rsqrt(total[:, 4:5] * (1.0 / (HEADS * VALUE_DIM)) + EPS)
    sides = []
    rows = other_out[2 * LANES :, :LANES].astype(F32)
    far = rows[0:4] + rows[4:8] + rows[8:12]
    for first, second, pooled, slot in (
        (gain_a[...], gain_p[...], pool_own, p),
        (far[0:1, :], far[1:2, :], pool_other, 1 - p),
    ):
        sides.append((attended[slot] * attention_factor * first).astype(BF16))
        sides.append((pooled[...] * pool_factor * second).astype(BF16))
    mine = jnp.concatenate(sides[:2], axis=1)
    theirs = jnp.concatenate(sides[2:], axis=1)
    step = 512
    for at in range(0, D, step):
        weights = jnp.concatenate(
            [own_attention[:, at : at + step], own_pool[:, at : at + step]], axis=0
        )
        both = dot(mine, weights) + dot(theirs, other_out[: 2 * LANES, at : at + step])
        partial_out[:, :, at : at + step] = both.astype(BF16).reshape(CHIPS, ROWS, step)


def sum_kernel(parts, out):
    total = parts[0].astype(F32) + parts[1].astype(F32)
    total = total + parts[2].astype(F32) + parts[3].astype(F32)
    out[0] = total.astype(BF16)


def local(
    tokens,
    input_gain,
    query_weight,
    latent_down,
    rotary_down,
    pool_down,
    key_up,
    value_up,
    query_gain,
    key_gain,
    pool_weight,
    pool_scale,
    attention_gain,
    pool_gain,
    attention_out,
    pool_out,
):
    inside, starts, turned, begins = (jnp.asarray(t) for t in angle_tables())

    def chip():
        return lax.axis_index("tp") // 2

    def up_to(step):
        return jnp.minimum(step, lax.axis_index("sp") // 4)

    normed, latent_rows, gain_row = whole(
        norm_kernel,
        (
            far((2 * CHIPS, ROWS, D), BF16),
            far((PACK, KV_LATENT), BF16),
            shape((8, LANES), F32),
        ),
        tokens,
        input_gain[None],
        latent_down,
        rotary_down.T,
        query_gain[None],
        room=56,
    )
    rows = among_all(normed)
    own_latents = lax.all_gather(latent_rows, "sp", axis=0, tiled=False)
    other_latents = to_partner(own_latents)

    queries, pool_rows, tail = whole(
        project_kernel,
        (
            far((2 * CHIPS, QROWS, LANES), BF16),
            far((BLOCK, LANES), BF16),
            far((HALO, LANES), BF16),
        ),
        rows,
        query_weight.T,
        pool_down,
        gain_row,
        inside,
        starts,
        specs=[AWAY] + [VECTOR] * 5,
        scratch=(
            pltpu.VMEM((2 * CHIPS, ROWS, D), BF16),
            pltpu.SemaphoreType.DMA((2,)),
        ),
        room=ROOM_PROJECT,
    )
    queries = among_all(queries)
    halo = lax.ppermute(tail, "sp", [(i, i + 1) for i in range(BLOCKS - 1)])

    latent_spec = pl.BlockSpec((4, PACK, KV_LATENT), lambda i: (up_to(i), 0, 0))
    expand = pl.pallas_call(
        expand_kernel,
        grid=(BLOCKS // 4,),
        out_shape=(far((HEADS, QK_DIM, KEYS), BF16), far((KEYS, KV_LATENT), BF16)),
        in_specs=[
            latent_spec,
            latent_spec,
            pl.BlockSpec((KV_LATENT, HEADS * NOPE_DIM), lambda i: (0, 0)),
            pl.BlockSpec((1, QK_DIM), lambda i: (0, 0)),
            pl.BlockSpec((2, 1, ROPE_DIM // 2, LANES), lambda i: (0, chip(), 0, 0)),
            pl.BlockSpec((2, 4, ROPE_DIM // 2, LANES), lambda i: (0, up_to(i), 0, 0)),
        ],
        out_specs=[
            pl.BlockSpec((HEADS, QK_DIM, QUAD), lambda i: (0, 0, up_to(i))),
            pl.BlockSpec((QUAD, KV_LATENT), lambda i: (up_to(i), 0)),
        ],
        scratch_shapes=[pltpu.VMEM((HEADS * NOPE_DIM, KV_LATENT), BF16)],
        compiler_params=pltpu.CompilerParams(vmem_limit_bytes=52 * MIB),
        name="expand",
    )
    keys, latents = expand(own_latents, other_latents, key_up, key_gain[None], turned, begins)

    numer = whole(
        attend_kernel,
        far((CHIPS, QROWS + HALO, 2 * LANES), BF16),
        queries,
        keys,
        latents,
        value_up,
        specs=[VECTOR, AWAY, AWAY, AWAY],
        outs=AWAY,
        scratch=(
            pltpu.VMEM((CHIPS, QROWS + HALO, 2 * LANES), BF16),
            pltpu.VMEM((HEADS, QK_DIM, KEYS), BF16),
            pltpu.VMEM((KEYS, KV_LATENT), BF16),
            pltpu.VMEM((KV_LATENT, HEADS * VALUE_DIM), BF16),
            pltpu.VMEM((HEADS, QROWS, KV_LATENT), F32),
            pltpu.VMEM((HEADS, QROWS, LANES), F32),
            pltpu.SemaphoreType.DMA((3, BLOCKS // 4 + 1)),
        ),
        room=53,
    )
    parts = among_chips(numer)

    pool_own, pool_give = whole(
        pool_kernel,
        (shape((QROWS, LANES), F32), shape((QROWS, LANES), F32)),
        pool_rows,
        halo,
        pool_weight,
        pool_scale[None],
    )
    pool_other = to_partner(pool_give)
    other_out = to_partner(
        whole(
            out_bundle_kernel,
            shape((2 * LANES + HALO, D), BF16),
            attention_out,
            pool_out,
            attention_gain[None],
            pool_gain[None],
        ),
    )
    attended, squares = whole(
        join_kernel,
        (shape((2, QROWS, LANES), F32), far((CHIPS, 8, QROWS), F32)),
        parts,
        pool_own,
        pool_other,
    )
    squares = among_chips(squares)
    partial = whole(
        mix_kernel,
        far((CHIPS, ROWS, D), BF16),
        attended,
        pool_own,
        pool_other,
        squares,
        attention_gain[None],
        pool_gain[None],
        attention_out,
        pool_out,
        other_out,
    )
    return whole(sum_kernel, shape((1, ROWS, D), BF16), among_chips(partial))


def solution(mesh):
    placed = (
        P("fs", ("sp", "tp"), None),
        P(),
        P(None, "tp"),
        P(),
        P(),
        P(None, "tp"),
        P(),
        P(),
        P(),
        P(),
        P(),
        P("tp"),
        P("tp"),
        P("tp"),
        P("tp", None),
        P("tp", None),
    )

    return jax.shard_map(
        local, mesh=mesh, in_specs=placed, out_specs=P("fs", ("sp", "tp"), None), check_vma=False
    )
```
